32 devices in a mesh: sp: 8 (over z, x), tp: 4 (over y, core).
Axes of the slice: x: 2, y: 2, z: 4, core: 2. Of those that a mesh axis runs over, the one named last changes fastest.
Arguments:
- residual: bfloat16 [6144, 2048], P('sp'), may hold values from -6 to 6
- query_matrix: bfloat16 [6144, 1024], P('sp', 'tp'), may hold values from -6 to 6
- key_matrix: bfloat16 [6144, 1024], P('sp', 'tp'), may hold values from -6 to 6
- value_matrix: bfloat16 [6144, 2048], P('sp', 'tp'), may hold values from -6 to 6
- output_gate_logit: bfloat16 [6144, 2048], P('sp', 'tp'), may hold values from -6 to 6
- input_gate_log: float32 [6144, 8], P('sp', 'tp'), may hold values from -4 to 125
- forget_gate_logit: float32 [6144, 8], P('sp', 'tp')
- extra_head_decay: float32 [6144, 8], P('sp', 'tp'), may hold values from -1 to 0
- head_norm_gain: float32 [2048], P('tp'), may hold values from 0.1 to 1.9
- projection: bfloat16 [2048, 2048], P('tp'), may hold values from -5.303301 to 5.303301
- cell_output_gain: float32 [2048], replicated, may hold values from 0.1 to 1.9
- mixer_input_gain: float32 [2048], replicated, may hold values from 0.1 to 1.9
- mixer_gate_weight: bfloat16 [2048, 5120], P('sp', 'tp'), may hold values from -0.125 to 0.125
- mixer_up_weight: bfloat16 [2048, 5120], P('sp', 'tp'), may hold values from -0.125 to 0.125
- mixer_down_weight: bfloat16 [5120, 2048], P('tp', 'sp'), may hold values from -0.078125 to 0.078125
Outputs:
- updated: bfloat16 [6144, 2048], P('sp', 'tp')
The draws below stay inside these ranges and needn't reach their ends.
All inputs are finite; a program needn't handle non-finite values.
Results may differ from the reference program's by a relative error of at most 0.014.
Values may be sent and summed in bfloat16 or wider, within the bound.
A program may use at most 128 MiB of HBM per device.

```python
import math
import jax
import jax.numpy as jnp
from jax import lax

D = 2048
HEADS = 8
DQK = 128
DV = 256
FF = 5120
TOK_DEV = 768
TOKENS = 6144
M_V = 2048
N_TP = 4


def draw_input_gate_log(key, part):
    values = jnp.clip(jax.random.normal(key, (TOKENS, HEADS), jnp.float32), -4.0, 4.0)
    return values


def draw_forget_gate_logit(key, part):
    slow_limit = 5
    slow = jax.random.randint(jax.random.fold_in(key, 1), (HEADS,), 0, 10) < slow_limit
    quick = jnp.log(jax.random.uniform(jax.random.fold_in(key, 2), (HEADS,), jnp.float32, 30.0, 60.0))
    level = jnp.where(slow, jnp.log(4.0 * TOKENS), quick)
    shifts = jax.random.uniform(jax.random.fold_in(key, 3), (TOKENS // TOK_DEV, HEADS), jnp.float32, -0.7, 0.7)
    shifts = jnp.repeat(shifts, TOK_DEV, axis=0)
    noise = jnp.clip(jax.random.normal(jax.random.fold_in(key, 4), (TOKENS, HEADS), jnp.float32), -4.0, 4.0)
    return level[None, :] + shifts + noise


def draw_extra_head_decay(key, part):
    spots = jax.random.randint(jax.random.fold_in(key, 1), (3, HEADS), 0, TOKENS)
    depth = jnp.log(jax.random.uniform(jax.random.fold_in(key, 2), (3, HEADS), jnp.float32, 0.5, 0.8))
    columns = lax.broadcasted_iota(jnp.int32, (3, HEADS), 1)
    return jnp.zeros((TOKENS, HEADS), jnp.float32).at[spots, columns].set(depth)


def draw_projection(key, part):
    base = jnp.clip(jax.random.normal(key, (M_V, D), jnp.float32), -6.0, 6.0) * M_V ** (-0.5)
    position = lax.broadcasted_iota(jnp.float32, (1, D), 1) / D
    jitter = jnp.exp(jax.random.uniform(jax.random.fold_in(key, 3), (1, D), jnp.float32, -0.35, 0.35))
    return (base * jnp.exp(1.0986 * position) * jitter).astype(jnp.bfloat16)


def level_of(rng, extent, shards, smallest, top_value):
    loudness = 1.0
    for axis_at, blocks in shards:
        steps = jax.random.uniform(jax.random.fold_in(jax.random.fold_in(rng, 6), axis_at), (blocks,), jnp.float32, smallest / len(shards), top_value / len(shards))
        loudness = loudness * jnp.repeat(jnp.exp(steps), extent[axis_at] // blocks).reshape((-1,) + (1,) * (len(extent) - 1 - axis_at))
    return loudness


def centred(stream_key, dims, scale, reach, cuts=(), kind=jnp.bfloat16):
    values = jax.random.normal(stream_key, dims, jnp.float32) * scale
    if len(cuts) > 0:
        values = level_of(stream_key, dims, cuts, -0.22, 0.18) * values
    return jnp.clip(values, min=-reach, max=reach).astype(kind)


def setup_inputs(seed: int = 0) -> dict:
    arg_keys = jax.random.split(jax.random.key(seed), 16)
    return {
        "residual": centred(arg_keys[0], (TOKENS, D), 1.0, 6.0, ((0, 8),)),
        "query_matrix": centred(arg_keys[1], (TOKENS, HEADS * DQK), 1.0, 6.0, ((0, 8), (1, 4))),
        "key_matrix": centred(arg_keys[2], (TOKENS, HEADS * DQK), 1.0, 6.0, ((0, 8), (1, 4))),
        "value_matrix": centred(arg_keys[3], (TOKENS, M_V), 1.0, 6.0, ((0, 8), (1, 4))),
        "output_gate_logit": centred(arg_keys[4], (TOKENS, M_V), 1.0, 6.0, ((0, 8), (1, 4))),
        "input_gate_log": draw_input_gate_log(jax.random.fold_in(arg_keys[15], 71), 0),
        "forget_gate_logit": draw_forget_gate_logit(jax.random.fold_in(arg_keys[15], 71), 0),
        "extra_head_decay": draw_extra_head_decay(jax.random.fold_in(arg_keys[15], 71), 0),
        "head_norm_gain": jnp.clip(1.0 + 0.18 * jax.random.normal(arg_keys[8], (M_V,), jnp.float32), 0.1, 1.9),
        "projection": draw_projection(jax.random.fold_in(arg_keys[15], 71), 0),
        "cell_output_gain": jnp.clip(1.0 + 0.18 * jax.random.normal(arg_keys[10], (D,), jnp.float32), 0.1, 1.9),
        "mixer_input_gain": jnp.clip(1.0 + 0.18 * jax.random.normal(arg_keys[11], (D,), jnp.float32), 0.1, 1.9),
        "mixer_gate_weight": centred(arg_keys[12], (D, FF), D ** -0.5, 0.125, ((0, 8), (1, 4))),
        "mixer_up_weight": centred(arg_keys[13], (D, FF), D ** -0.5, 0.125, ((0, 8), (1, 4))),
        "mixer_down_weight": centred(arg_keys[14], (FF, D), FF ** -0.5, 0.078125, ((0, 4), (1, 8))),
    }


HIGHEST = lax.Precision.HIGHEST
EPSILON = 1e-06

def read_out(query, keyed, valued, in_logs, running_log_total, memory, normalizer, stabilizer):
    length = query.shape[1]
    causal = lax.broadcasted_iota(jnp.int32, (length, length), 0) >= lax.broadcasted_iota(jnp.int32, (length, length), 1)
    spread = running_log_total[:, :, None] - running_log_total[:, None, :] + in_logs[:, None, :]
    spread = jnp.where(causal[None], spread, -jnp.inf)
    carried = running_log_total + stabilizer[:, None]
    running = jnp.maximum(carried, lax.optimization_barrier(jnp.max(spread, axis=-1)))
    scores = jnp.einsum('htd,hsd->hts', query, keyed, precision=HIGHEST) * DQK ** (-0.5)
    weights = jnp.exp(spread - running[:, :, None]) * scores
    weight_low = lax.optimization_barrier(weights.astype(jnp.bfloat16)).astype(jnp.float32)
    scaled = jnp.exp(carried - running)
    scaled_query = query * DQK ** (-0.5)
    numerator = jnp.einsum('hts,hsv->htv', weight_low, valued, precision=HIGHEST)
    numerator = numerator + scaled[:, :, None] * jnp.einsum('hvd,htd->htv', memory, scaled_query, precision=HIGHEST)
    denominator = lax.optimization_barrier(jnp.sum(weights, axis=-1)) + scaled * jnp.einsum('hd,htd->ht', normalizer, scaled_query, precision=HIGHEST)
    return numerator / jnp.maximum(jnp.abs(denominator), jnp.exp(-running))[:, :, None]

def fold_state(keyed, valued, in_logs, running_log_total, memory, normalizer, stabilizer):
    last = running_log_total[:, -1]
    lifted = last[:, None] - running_log_total + in_logs
    new_max = jnp.maximum(last + stabilizer, lax.optimization_barrier(jnp.max(lifted, axis=-1)))
    weights = jnp.exp(lifted - new_max[:, None])
    retained = jnp.exp(last + stabilizer - new_max)
    memory = retained[:, None, None] * memory + jnp.einsum('hsv,hsd->hvd', weights[:, :, None] * valued, keyed, precision=HIGHEST)
    normalizer = retained[:, None] * normalizer + jnp.einsum('hs,hsd->hd', weights, keyed, precision=HIGHEST)
    return (memory, normalizer, new_max)

def block_sum(left, right, parts):
    rows = left.shape[0]
    inner = left.shape[1] // parts
    left_blocks = left.reshape(rows, parts, inner).transpose(1, 0, 2)
    right_blocks = right.reshape(parts, inner, right.shape[1])

    def accumulate(total, pair):
        product = jnp.dot(pair[0], pair[1], preferred_element_type=jnp.float32).astype(jnp.bfloat16)
        return (total + lax.optimization_barrier(product).astype(jnp.float32), None)
    total, unused = lax.scan(accumulate, jnp.zeros((rows, right.shape[1]), jnp.float32), (left_blocks, right_blocks))
    return total

def reference(residual, query_matrix, key_matrix, value_matrix, output_gate_logit, input_gate_log, forget_gate_logit, extra_head_decay, head_norm_gain, projection, cell_output_gain, mixer_input_gain, mixer_gate_weight, mixer_up_weight, mixer_down_weight):
    span = math.gcd(TOKENS, 512)
    count = TOKENS // span

    def arrange(array, width):
        return array.astype(jnp.float32).reshape(count, span, HEADS, width).transpose(0, 2, 1, 3)
    query = arrange(query_matrix, DQK)
    keyed = arrange(key_matrix, DQK)
    valued = arrange(value_matrix, DV)
    in_logs = input_gate_log.reshape(count, span, HEADS).transpose(0, 2, 1)
    forget_log_value = jax.nn.log_sigmoid(forget_gate_logit) + extra_head_decay
    running_log_total = jnp.cumsum(forget_log_value.reshape(count, span, HEADS), axis=1).transpose(0, 2, 1)

    def advance(state, blocks):
        memory, normalizer, stabilizer = state
        query_block, key_block, value_block, gate_block, decay_block = blocks
        cells = read_out(query_block, key_block, value_block, gate_block, decay_block, memory, normalizer, stabilizer)
        return (fold_state(key_block, value_block, gate_block, decay_block, memory, normalizer, stabilizer), cells)
    start = (jnp.zeros((HEADS, DV, DQK), jnp.float32), jnp.zeros((HEADS, DQK), jnp.float32), jnp.zeros((HEADS,), jnp.float32))
    unused, cells = lax.scan(advance, start, (query, keyed, valued, in_logs, running_log_total))
    centered = cells - lax.optimization_barrier(jnp.mean(cells, axis=-1, keepdims=True))
    normed = centered * lax.rsqrt(lax.optimization_barrier(jnp.mean(centered * centered, axis=-1, keepdims=True)) + EPSILON)
    normed = normed * head_norm_gain.reshape(HEADS, DV)[None, :, None, :]
    normed = normed.transpose(0, 2, 1, 3).reshape(TOKENS, HEADS * DV)
    gated = (normed * jax.nn.sigmoid(output_gate_logit.astype(jnp.float32))).astype(jnp.bfloat16)
    mixed = block_sum(gated, projection, N_TP)
    mixed = mixed * lax.rsqrt(lax.optimization_barrier(jnp.mean(mixed * mixed, axis=-1, keepdims=True)) + EPSILON) * cell_output_gain
    first_sum = (residual.astype(jnp.float32) + mixed).astype(jnp.bfloat16)
    first_wide = lax.optimization_barrier(first_sum).astype(jnp.float32)
    normed_rows = (first_wide * lax.rsqrt(lax.optimization_barrier(jnp.mean(first_wide * first_wide, axis=-1, keepdims=True)) + EPSILON) * mixer_input_gain).astype(jnp.bfloat16)
    gate_value = jnp.dot(normed_rows, mixer_gate_weight, preferred_element_type=jnp.float32)
    up_value = jnp.dot(normed_rows, mixer_up_weight, preferred_element_type=jnp.float32)
    activated = (jax.nn.silu(gate_value) * up_value).astype(jnp.bfloat16)
    channel_out = block_sum(activated, mixer_down_weight, N_TP)
    return (first_wide + 0.5 * channel_out).astype(jnp.bfloat16)
```

```python
import functools

import jax
import jax.numpy as jnp
from jax import lax
from jax.experimental import pallas as pl
from jax.experimental.pallas import tpu as pltpu
from jax.sharding import PartitionSpec as P

DQK = 128
DV = 256
MESH = pl.DeviceIdType.MESH
VMEM = pl.BlockSpec(memory_space=pltpu.VMEM)
ANY = pl.BlockSpec(memory_space=pl.ANY)
VMEM_BYTES = 62 * 1024 * 1024

HIGHEST = lax.Precision.HIGHEST
EPSILON = 1e-06
LOWEST_LOG = -1e30


def heads_first(array, heads, width):
    return array.reshape(array.shape[0], heads, width).transpose(1, 0, 2)


def fold_state(keyed, valued, in_logs, running_log_total, memory, normalizer, stabilizer):
    last = running_log_total[:, -1]
    lifted = last[:, None] - running_log_total + in_logs
    new_max = jnp.maximum(last + stabilizer, jnp.max(lifted, axis=-1))
    weights = jnp.exp(lifted - new_max[:, None])
    retained = jnp.exp(last + stabilizer - new_max)
    memory = retained[:, None, None] * memory + jnp.einsum(
        "hsv,hsd->hvd", weights[:, :, None] * valued, keyed, precision=HIGHEST
    )
    normalizer = retained[:, None] * normalizer + jnp.einsum(
        "hs,hsd->hd", weights, keyed, precision=HIGHEST
    )
    return (memory, normalizer, new_max)


def copy_to(source, target, sems, slot, peer):
    return pltpu.make_async_remote_copy(
        source, target, sems.at[(0, *slot)], sems.at[(1, *slot)], device_id=peer, device_id_type=MESH
    )


def layer_kernel(
    ranks, count, heads, memory_ref, aux_ref, cum_row, in_row, cum_col, query_ref,
    key_ref, value_ref, ogate_ref, head_gain, residual_ref, out_gain, in_gain, projection_ref,
    gate_ref, up_ref, down_ref, out_ref, slots, aux_slots, memory, aux, gate_w, up_w, down_w,
    weight, gated, blocks, normed, first, active, to_core, from_core, to_chip, from_chip,
    state_sems, aux_sems, local_sems, proj_sems, gated_sems, sum_sems,
):
    sp, me = lax.axis_index("sp"), lax.axis_index("tp")
    core = lax.rem(me, 2)
    mate = me + 1 - 2 * core
    chips = count // 2
    rows_all, width = residual_ref.shape
    cols = out_ref.shape[1]
    inner = value_ref.shape[1]

    barrier = pltpu.get_barrier_semaphore()
    for axis, size, at in (("sp", ranks, sp), ("tp", count, me)):
        for step in range(1, size):
            pl.semaphore_signal(
                barrier, inc=1, device_id={axis: lax.rem(at + step, size)}, device_id_type=MESH
            )
    pl.semaphore_wait(barrier, ranks + count - 2)

    def state_copies(step):
        peer = {"sp": lax.rem(sp + step, ranks)}
        return (
            copy_to(memory_ref, slots.at[step - 1], state_sems, (step - 1,), peer),
            copy_to(aux_ref, aux_slots.at[step - 1], aux_sems, (step - 1,), peer),
        )

    for step in range(1, ranks):

        @pl.when(sp + step < ranks)
        def _():
            for copy in state_copies(step):
                copy.start()

    def spread(source, whole, sems):
        sent = [copy_to(source, whole.at[me], sems, (0,), {"tp": mate})]
        for step in range(1, chips):
            peer = {"tp": lax.rem(me + 2 * step, count)}
            sent.append(copy_to(source, whole.at[me], sems, (2 * step,), peer))
        for copy in sent:
            copy.start()
        return sent

    def relay(whole, sems):
        sent = []
        for step in range(1, chips):
            owner = lax.rem(me - 2 * step + count, count)
            block = whole.at[owner]
            copy_to(block, block, sems, (2 * step,), {"tp": mate}).wait_recv()
            sent.append(copy_to(block, block, sems, (2 * step - 1,), {"tp": mate}))
            sent[-1].start()
        return sent

    def collect(whole, sems):
        for step in range(chips):
            owner = lax.rem(mate - 2 * step + count, count)
            block = whole.at[owner]
            slot = 0 if step == 0 else 2 * step - 1
            copy_to(block, block, sems, (slot,), {"tp": mate}).wait_recv()

    for ref, whole, at in ((gate_ref, gate_w, 0), (up_ref, up_w, 1)):
        pltpu.make_async_copy(ref, whole, local_sems.at[at]).start()
    pltpu.make_async_copy(down_ref, down_w.at[0], local_sems.at[2]).start()
    own_weight = pltpu.make_async_copy(projection_ref, weight.at[me], local_sems.at[4])
    own_weight.start()
    sent = spread(projection_ref, weight, proj_sems)

    memory[...] = jnp.zeros_like(memory)
    aux[...] = jnp.zeros_like(aux)
    aux[heads : 2 * heads, :] = jnp.full((heads, DQK), LOWEST_LOG, jnp.float32)
    for step in range(ranks - 1, 0, -1):

        @pl.when(sp >= step)
        def _():
            for copy in state_copies(step):
                copy.wait_recv()
            late = aux_slots[step - 1]
            for head in range(heads):
                rows = pl.ds(head * DV, DV)
                early_max = aux[heads + head : heads + head + 1, :]
                late_max = late[heads + head : heads + head + 1, :]
                late_decay = late[2 * heads + head : 2 * heads + head + 1, :]
                joined = jnp.maximum(late_decay + early_max, late_max)
                before = jnp.exp(late_decay + early_max - joined)
                after = jnp.exp(late_max - joined)
                memory[rows, :] = before * memory[rows, :] + after * slots[
                    step - 1, rows, :
                ].astype(jnp.float32)
                aux[head : head + 1, :] = (
                    before * aux[head : head + 1, :] + after * late[head : head + 1, :]
                )
                aux[heads + head : heads + head + 1, :] = joined
                aux[2 * heads + head : 2 * heads + head + 1, :] = (
                    aux[2 * heads + head : 2 * heads + head + 1, :] + late_decay
                )

    tile = rows_all // 3
    for head in range(heads):
        prior_max = aux[heads + head : heads + head + 1, :]
        start_max = jnp.maximum(aux[2 * heads + head : 2 * heads + head + 1, :], prior_max)
        lift = jnp.exp(prior_max - start_max) * DQK ** (-0.5)
        memory[head * DV : (head + 1) * DV, :] = memory[head * DV : (head + 1) * DV, :] * lift
        aux[head : head + 1, :] = aux[head : head + 1, :] * lift
        aux[2 * heads + head : 2 * heads + head + 1, :] = start_max

    def read(at, unused):
        start = pl.multiple_of(at * tile, tile)
        rows = pl.ds(start, tile)
        causal = start + lax.broadcasted_iota(
            jnp.int32, (tile, rows_all), 0
        ) >= lax.broadcasted_iota(jnp.int32, (tile, rows_all), 1)
        for head in range(heads):
            keys = slice(head * DQK, (head + 1) * DQK)
            values = slice(head * DV, (head + 1) * DV)
            query = query_ref[rows, keys]
            total = cum_col[rows, head : head + 1]
            spread_log = total - cum_row[head : head + 1, :] + in_row[head : head + 1, :]
            spread_log = jnp.where(causal, spread_log, -jnp.inf)
            carried = total + aux[2 * heads + head : 2 * heads + head + 1, :1]
            running = jnp.maximum(carried, jnp.max(spread_log, axis=-1, keepdims=True))
            scores = lax.dot_general(
                query, key_ref[:, keys], (((1,), (1,)), ((), ())),
                preferred_element_type=jnp.float32,
            ) * DQK ** (-0.5)
            weights = jnp.exp(spread_log - running) * scores
            scaled = jnp.exp(carried - running)
            wide = query.astype(jnp.float32)
            numerator = jnp.dot(
                weights.astype(jnp.bfloat16), value_ref[:, values],
                preferred_element_type=jnp.float32,
            ) + scaled * lax.dot_general(
                wide, memory[values, :], (((1,), (1,)), ((), ())), precision=HIGHEST,
                preferred_element_type=jnp.float32,
            )
            denominator = jnp.sum(weights, axis=-1, keepdims=True) + scaled * jnp.sum(
                wide * aux[head : head + 1, :], axis=-1, keepdims=True
            )
            cell = numerator / jnp.maximum(jnp.abs(denominator), jnp.exp(-running))
            centered = cell - jnp.mean(cell, axis=-1, keepdims=True)
            cell = centered * lax.rsqrt(
                jnp.mean(centered * centered, axis=-1, keepdims=True) + EPSILON
            )
            cell = cell * head_gain[:, values]
            gate = ogate_ref[rows, values].astype(jnp.float32)
            gated[rows, values] = (cell * jax.nn.sigmoid(gate)).astype(jnp.bfloat16)
        return unused

    lax.fori_loop(0, 3, read, 0)
    sent += spread(gated, blocks, gated_sems)
    blocks[me] = gated[...]
    sent += relay(weight, proj_sems)
    sent += relay(blocks, gated_sems)
    collect(weight, proj_sems)
    own_weight.wait()
    collect(blocks, gated_sems)

    def turn(at, unused):
        rows = pl.ds(pl.multiple_of(at * tile, tile), tile)
        mixed = jnp.zeros((tile, width), jnp.float32)
        for block in range(count):
            mixed = mixed + jnp.dot(
                blocks[block, rows, :], weight[block], preferred_element_type=jnp.float32
            )
        scale = lax.rsqrt(jnp.mean(mixed * mixed, axis=-1, keepdims=True) + EPSILON)
        total = residual_ref[rows, :].astype(jnp.float32) + mixed * scale * out_gain[...]
        total = total.astype(jnp.bfloat16)
        first[rows, :] = total
        wide = total.astype(jnp.float32)
        scale = lax.rsqrt(jnp.mean(wide * wide, axis=-1, keepdims=True) + EPSILON)
        normed[rows, :] = (wide * scale * in_gain[...]).astype(jnp.bfloat16)
        return unused

    lax.fori_loop(0, 3, turn, 0)

    for ref, whole, at in ((gate_ref, gate_w, 0), (up_ref, up_w, 1)):
        pltpu.make_async_copy(ref, whole, local_sems.at[at]).wait()

    def mix(at, unused):
        rows = pl.ds(pl.multiple_of(at * tile, tile), tile)
        left = normed[rows, :]
        gate = jnp.dot(left, gate_w[...], preferred_element_type=jnp.float32)
        up = jnp.dot(left, up_w[...], preferred_element_type=jnp.float32)
        active[rows, :] = (gate / (1.0 + jnp.exp(-gate)) * up).astype(jnp.bfloat16)
        return unused

    lax.fori_loop(0, 3, mix, 0)
    pltpu.make_async_copy(down_ref, down_w.at[0], local_sems.at[2]).wait()

    def term(target):
        start = pl.multiple_of(target * cols, cols)
        return jnp.dot(
            active[...], down_w[0, :, pl.ds(start, cols)], preferred_element_type=jnp.float32
        )

    def send(source, target, kind, at, peer):
        return copy_to(source.at[at], target.at[at], sum_sems.at[kind], (at,), {"tp": peer})

    copies = []
    for step in range(1, chips):
        away = lax.rem(me + 2 * step, count)
        to_core[step] = term(away + 1 - 2 * core).astype(jnp.bfloat16)
        hop = send(to_core, from_core, 0, step, mate)
        hop.start()
        mine = term(away)
        hop.wait_recv()
        to_chip[step] = (mine + from_core[step].astype(jnp.float32)).astype(jnp.bfloat16)
        far = send(to_chip, from_chip, 1, step, away)
        far.start()
        copies += [hop, far]
    to_core[0] = term(mate).astype(jnp.bfloat16)
    hop = send(to_core, from_core, 0, 0, mate)
    hop.start()
    result = term(me)
    hop.wait_recv()
    result = result + from_core[0].astype(jnp.float32)
    for far in copies[1::2]:
        far.wait_recv()
    for step in range(1, chips):
        result = result + from_chip[step].astype(jnp.float32)
    own_first = first[:, pl.ds(pl.multiple_of(me * cols, cols), cols)]
    out_ref[...] = (own_first.astype(jnp.float32) + 0.5 * result).astype(jnp.bfloat16)
    for copy in copies + [hop] + sent:
        copy.wait_send()
    for step in range(1, ranks):

        @pl.when(sp + step < ranks)
        def _():
            for copy in state_copies(step):
                copy.wait_send()


def layer(states, logs, cell_inputs, residual, gains, weights):
    decay, memory, normalizer, maximum = states
    running_log_total, in_logs = logs
    ranks, count = lax.axis_size("sp"), lax.axis_size("tp")
    heads = decay.shape[0]
    rows, width = residual.shape
    projection, gate_weight, up_weight, down_weight = weights
    hidden = gate_weight.shape[1]
    inner = projection.shape[0]
    gate_weight = lax.all_gather(gate_weight, "sp", axis=0, tiled=True)
    up_weight = lax.all_gather(up_weight, "sp", axis=0, tiled=True)
    down_weight = lax.all_gather(down_weight, "sp", axis=1, tiled=True)
    down_shape = (1, hidden, width)
    fill = lambda row: jnp.broadcast_to(row[:, None], (heads, DQK))
    aux = jnp.concatenate([normalizer, fill(maximum), fill(decay)])
    height = -(-3 * heads // 8) * 8
    aux = jnp.pad(aux, ((0, height - 3 * heads), (0, 0)))
    low = memory.reshape(heads * DV, DQK).astype(jnp.bfloat16)
    chips, cols = count // 2, width // count
    buffer = pltpu.VMEM((chips, rows, cols), jnp.bfloat16)
    dma = pltpu.SemaphoreType.DMA
    return pl.pallas_call(
        functools.partial(layer_kernel, ranks, count, heads),
        out_shape=jax.ShapeDtypeStruct((rows, cols), jnp.bfloat16),
        in_specs=[VMEM] * 13 + [ANY] * 4,
        out_specs=VMEM,
        scratch_shapes=[
            pltpu.VMEM((ranks - 1, heads * DV, DQK), jnp.bfloat16),
            pltpu.VMEM((ranks - 1, height, DQK), jnp.float32),
            pltpu.VMEM((heads * DV, DQK), jnp.float32),
            pltpu.VMEM((height, DQK), jnp.float32),
            pltpu.VMEM((width, hidden), jnp.bfloat16),
            pltpu.VMEM((width, hidden), jnp.bfloat16),
            pltpu.VMEM(down_shape, jnp.bfloat16),
            pltpu.VMEM((count, inner, width), jnp.bfloat16),
            pltpu.VMEM((rows, inner), jnp.bfloat16),
            pltpu.VMEM((count, rows, inner), jnp.bfloat16),
            pltpu.VMEM((rows, width), jnp.bfloat16),
            pltpu.VMEM((rows, width), jnp.bfloat16),
            pltpu.VMEM((rows, hidden), jnp.bfloat16),
            buffer, buffer, buffer, buffer,
            dma((2, ranks - 1)),
            dma((2, ranks - 1)),
            dma((5,)),
            dma((2, count)),
            dma((2, count)),
            dma((2, 2, chips)),
        ],
        compiler_params=pltpu.CompilerParams(
            collective_id=0, has_side_effects=True, vmem_limit_bytes=VMEM_BYTES
        ),
        name="layer",
    )(
        low, aux, running_log_total, in_logs, running_log_total.T, *cell_inputs, residual,
        *gains, projection, gate_weight, up_weight, down_weight,
    )


def pair_kernel(
    ranks, count, heads, forget_hbm, extra_hbm, in_hbm, query_hbm, key_hbm, value_hbm, ogate_hbm,
    head_gain_hbm, residual_hbm, out_gain_hbm, in_gain_hbm, projection_hbm, gate_hbm, up_hbm,
    down_hbm, out_ref, forget, extra, in_row, query, key, value, ogate, head_gain, residual,
    out_gain, in_gain, proj_own, proj_mate, gate_w, up_w, down_w, cum_row, cols, own_mem, mem_send,
    aux, x_mem, x_aux, e_mem, e_aux, t_mem, t_aux, z_mem, z_aux, p_mem, p_aux, q_mem, q_aux,
    final_mem, final_aux, local, gated, mate_gated, part_send, part_recv, acc, first_own,
    first_cols, normed, active, to_core, from_core, y_send, y_recv, z_send, z_recv, held, kept,
    local_sems, w_sems, state_sems, line_sems, mate_sems, part_sems, ag_sems, first_sems,
    core_sems, link_sems,
):
    sp, me = lax.axis_index("sp"), lax.axis_index("tp")
    row, col = sp // 2, lax.rem(sp, 2)
    depth = ranks // 2
    par = lax.rem(row, 2)
    core = lax.rem(me, 2)
    chip = me // 2
    mate = me + 1 - 2 * core
    across = lax.rem(me + 2, count)
    corner = lax.rem(mate + 2, count)
    rows_all, width = out_ref.shape[0], out_gain.shape[1]
    cols_out = out_ref.shape[1]
    block = rows_all // count
    half = gate_w.shape[1]
    high = gate_hbm.shape[0]
    others = {1: row + 1 - 2 * par, 2: lax.rem(row + 2, depth), 3: depth - 1 - row}
    to_x = {"sp": row * 2 + 1 - col}
    to_z = {"sp": others[1] * 2 + col}
    to_mate, to_y = {"tp": mate}, {"tp": across}
    sent = []

    barrier = pltpu.get_barrier_semaphore()
    greeted = [{"sp": others[i] * 2 + col} for i in (1, 2, 3)]
    greeted += [to_x, to_mate, to_y, {"tp": corner}]
    for peer in greeted:
        pl.semaphore_signal(barrier, inc=1, device_id=peer, device_id_type=MESH)

    loads = {}

    def load(name, source, target):
        loads[name] = pltpu.make_async_copy(source, target, local_sems.at[len(loads)])
        loads[name].start()

    load("forget", forget_hbm, forget)
    load("extra", extra_hbm, extra)
    load("in", in_hbm, in_row)
    load("key", key_hbm, key)
    load("value", value_hbm, value)
    load("query", query_hbm, query)
    load("ogate", ogate_hbm, ogate)
    load("head", head_gain_hbm, head_gain)
    load("proj", projection_hbm, proj_own)
    own_rows = pl.ds(pl.multiple_of(me * block, block), block)
    load("residual", residual_hbm.at[own_rows, :], residual)
    load("outg", out_gain_hbm, out_gain)
    load("ing", in_gain_hbm, in_gain)

    def piece(kind, parity):
        at = pl.ds(pl.multiple_of(parity * half, half), half)
        if kind == 2:
            return down_hbm.at[at, :]
        return (gate_hbm, up_hbm)[kind].at[:, at]

    def place(kind, owner):
        if kind == 2:
            return down_w.at[owner]
        at = pl.ds(pl.multiple_of(owner * high, high), high)
        return (gate_w, up_w)[kind].at[at, :]

    for kind in range(3):
        load(kind, piece(kind, par), place(kind, sp))

    pl.semaphore_wait(barrier, len(greeted))

    def send(source, target, sems, slot, peer):
        copy = copy_to(source, target, sems, slot, peer)
        copy.start()
        sent.append(copy)

    def arrived(target, sems, slot):
        copy_to(target, target, sems, slot, to_mate).wait_recv()

    def z_weights(kind, i):
        there = others[i]
        send(
            piece(kind, lax.rem(there, 2)), place(kind, sp), w_sems, (kind, 0, i),
            {"sp": there * 2 + col},
        )

    def x_weights(kind):
        send(piece(kind, par), place(kind, sp), w_sems, (kind, 1, 0), to_x)

    relays = [(kind, i) for kind in range(3) for i in (1, 3, 2)]

    def pump(number):
        for _ in range(number):
            kind, i = relays.pop(0)
            spot = place(kind, others[i] * 2 + col)
            arrived(spot, w_sems, (kind, 0, i))
            send(spot, spot, w_sems, (kind, 1, i), to_x)

    def gathered(kind):
        loads[kind].wait()
        for i in range(depth):
            there = row if i == 0 else others[i]
            arrived(place(kind, there * 2 + 1 - col), w_sems, (kind, 1, i))

    z_weights(0, 1)
    send(projection_hbm, proj_mate, mate_sems, (2,), to_mate)

    for name in ("forget", "extra", "in"):
        loads[name].wait()
    logit = forget[...]
    decay = jnp.minimum(logit, 0.0) - jnp.log1p(jnp.exp(-jnp.abs(logit))) + extra[...]
    lane = lax.broadcasted_iota(jnp.int32, decay.shape, 1)
    shift = 1
    while shift < rows_all:
        decay = decay + jnp.where(lane >= shift, pltpu.roll(decay, shift, 1), 0.0)
        shift *= 2
    cum_row[...] = decay
    last = decay[:, rows_all - 1 : rows_all]
    lifted = last - decay + in_row[...]
    top = jnp.max(lifted, axis=-1, keepdims=True)
    lifted = jnp.exp(lifted - top)
    eye = lax.broadcasted_iota(jnp.int32, (128, 128), 0) == lax.broadcasted_iota(
        jnp.int32, (128, 128), 1
    )

    def to_column(line, at):
        for start in range(0, rows_all, 128):
            spread = jnp.broadcast_to(line[:, start : start + 128], (128, 128))
            cols[start : start + 128, at : at + 1] = jnp.sum(
                jnp.where(eye, spread, 0.0), axis=-1, keepdims=True
            )

    for head in range(heads):
        to_column(decay[head : head + 1, :], head)
        to_column(lifted[head : head + 1, :], heads + head)
    loads["key"].wait()
    loads["value"].wait()
    for head in range(heads):
        keys = slice(head * DQK, (head + 1) * DQK)
        values = slice(head * DV, (head + 1) * DV)
        share = cols[:, heads + head : heads + head + 1]
        heavy = (share * value[:, values].astype(jnp.float32)).astype(jnp.bfloat16)
        state = lax.dot_general(
            key[:, keys], heavy, (((0,), (0,)), ((), ())), preferred_element_type=jnp.float32
        )
        own_mem[head] = state
        mem_send[head] = state.astype(jnp.bfloat16)
        aux[head] = jnp.zeros((8, DQK), jnp.float32)
        aux[head, 0:1, :] = jnp.sum(
            share * key[:, keys].astype(jnp.float32), axis=0, keepdims=True
        )
        aux[head, 1:2, :] = jnp.broadcast_to(top[head : head + 1, :], (1, DQK))
        aux[head, 2:3, :] = jnp.broadcast_to(last[head : head + 1, :], (1, DQK))
    send(mem_send.at[1 - col], x_mem, state_sems, (0,), to_x)
    send(aux.at[1 - col], x_aux, state_sems, (1,), to_x)
    x_weights(0)

    tile = rows_all // 3
    loads["query"].wait()

    def nearby(head, at):
        start, reach = at * tile, (at + 1) * tile
        keys = slice(head * DQK, (head + 1) * DQK)
        values = slice(head * DV, (head + 1) * DV)
        rows = slice(start, reach)
        causal = start + lax.broadcasted_iota(
            jnp.int32, (tile, reach), 0
        ) >= lax.broadcasted_iota(jnp.int32, (tile, reach), 1)
        total = cols[rows, head : head + 1]
        spread_log = total - cum_row[head : head + 1, :reach] + in_row[head : head + 1, :reach]
        spread_log = jnp.where(causal, spread_log, -jnp.inf)
        running = jnp.max(spread_log, axis=-1, keepdims=True)
        scores = lax.dot_general(
            query[rows, keys], key[:reach, keys], (((1,), (1,)), ((), ())),
            preferred_element_type=jnp.float32,
        ) * DQK ** (-0.5)
        weights = jnp.exp(spread_log - running) * scores
        local[rows, values] = jnp.dot(
            weights.astype(jnp.bfloat16), value[:reach, values],
            preferred_element_type=jnp.float32,
        )
        cols[rows, 2 * heads + head : 2 * heads + head + 1] = running
        cols[rows, 3 * heads + head : 3 * heads + head + 1] = jnp.sum(
            weights, axis=-1, keepdims=True
        )

    nearby(0, 0)
    nearby(1, 0)
    nearby(0, 1)

    def parts(ref):
        return ref[0:1, :], ref[1:2, :], ref[2:3, :]

    def join(early_mem, early, late_mem, late):
        joined = jnp.maximum(late[2] + early[1], late[1])
        before = jnp.exp(late[2] + early[1] - joined)
        after = jnp.exp(late[1] - joined)
        memory = before[:, :1] * early_mem + after[:, :1] * late_mem
        return memory, (before * early[0] + after * late[0], joined, early[2] + late[2])

    def keep(ref, values):
        ref[...] = jnp.zeros(ref.shape, jnp.float32)
        for at, entry in enumerate(values):
            ref[at : at + 1, :] = entry

    left = col == 0
    arrived(x_mem, state_sems, (0,))
    arrived(x_aux, state_sems, (1,))
    mine, theirs = own_mem[col], x_mem[...].astype(jnp.float32)
    mine_aux = tuple(aux[col, at : at + 1, :] for at in range(3))
    theirs_aux = parts(x_aux)
    pick = lambda one, two: jnp.where(left, one, two)
    early_mem, late_mem = pick(mine, theirs), pick(theirs, mine)
    early_aux = tuple(pick(one, two) for one, two in zip(mine_aux, theirs_aux))
    late_aux = tuple(pick(two, one) for one, two in zip(mine_aux, theirs_aux))
    e_mem[...] = early_mem
    keep(e_aux, early_aux)
    both, both_aux = join(early_mem, early_aux, late_mem, late_aux)
    t_mem[...] = both.astype(jnp.bfloat16)
    keep(t_aux, both_aux)

    def plane_copies(step):
        peer = {"sp": lax.rem(sp + 2 * step, ranks)}
        return (
            copy_to(t_mem, z_mem.at[step - 1], line_sems, (0, step - 1), peer),
            copy_to(t_aux, z_aux.at[step - 1], line_sems, (1, step - 1), peer),
        )

    for step in range(1, depth):

        @pl.when(row + step < depth)
        def _():
            for copy in plane_copies(step):
                copy.start()

    for kind in (0, 1):
        for i in (3, 2, 1):
            if (kind, i) != (0, 1):
                z_weights(kind, i)
    nearby(1, 1)
    nearby(0, 2)
    nearby(1, 2)

    p_mem[...] = jnp.zeros(p_mem.shape, jnp.float32)
    zero = jnp.zeros((1, DQK), jnp.float32)
    keep(p_aux, (zero, jnp.full((1, DQK), LOWEST_LOG, jnp.float32), zero))
    for step in range(depth - 1, 0, -1):

        @pl.when(row >= step)
        def _():
            for copy in plane_copies(step):
                copy.wait_recv()
            memory, rest = join(
                p_mem[...], parts(p_aux), z_mem[step - 1].astype(jnp.float32),
                parts(z_aux.at[step - 1]),
            )
            p_mem[...] = memory
            keep(p_aux, rest)

    prior, prior_aux = p_mem[...], parts(p_aux)
    more, more_aux = join(prior, prior_aux, e_mem[...], parts(e_aux))
    q_mem[...] = pick(more, prior).astype(jnp.bfloat16)
    keep(q_aux, tuple(pick(one, two) for one, two in zip(more_aux, prior_aux)))
    send(q_mem, final_mem.at[col], state_sems, (2,), to_x)
    send(q_aux, final_aux.at[col], state_sems, (3,), to_x)
    x_weights(1)
    final_mem[col] = pick(prior, more).astype(jnp.bfloat16)
    keep(final_aux.at[col], tuple(pick(two, one) for one, two in zip(more_aux, prior_aux)))
    pump(1)
    loads["ogate"].wait()
    loads["head"].wait()
    arrived(final_mem.at[1 - col], state_sems, (2,))
    arrived(final_aux.at[1 - col], state_sems, (3,))

    for head in range(heads):
        keys = slice(head * DQK, (head + 1) * DQK)
        values = slice(head * DV, (head + 1) * DV)
        prior_max = final_aux[head, 1:2, :]
        start_max = jnp.maximum(final_aux[head, 2:3, :], prior_max)
        lift = (jnp.exp(prior_max - start_max) * DQK ** (-0.5))[:, :1]
        start_max = start_max[:, :1]
        for at in range(3):
            rows = slice(at * tile, (at + 1) * tile)
            question = query[rows, keys]
            found = cols[rows, 2 * heads + head : 2 * heads + head + 1]
            carried = cols[rows, head : head + 1] + start_max
            running = jnp.maximum(carried, found)
            inside = jnp.exp(found - running)
            scaled = jnp.exp(carried - running) * lift
            numerator = inside * local[rows, values] + scaled * jnp.dot(
                question, final_mem[head], preferred_element_type=jnp.float32
            )
            denominator = inside * cols[
                rows, 3 * heads + head : 3 * heads + head + 1
            ] + scaled * jnp.sum(
                question.astype(jnp.float32) * final_aux[head, 0:1, :], axis=-1, keepdims=True
            )
            cell = numerator / jnp.maximum(jnp.abs(denominator), jnp.exp(-running))
            centered = cell - jnp.mean(cell, axis=-1, keepdims=True)
            cell = centered * lax.rsqrt(
                jnp.mean(centered * centered, axis=-1, keepdims=True) + EPSILON
            )
            gate = ogate[rows, values].astype(jnp.float32)
            gated[rows, values] = (
                cell * head_gain[:, values] * jax.nn.sigmoid(gate)
            ).astype(jnp.bfloat16)

    def rows_of(owner):
        return pl.ds(pl.multiple_of(owner * block, block), block)

    send(gated.at[rows_of(corner), :], mate_gated.at[0], mate_sems, (0,), to_mate)
    send(gated.at[rows_of(mate), :], mate_gated.at[1], mate_sems, (1,), to_mate)
    loads["proj"].wait()
    arrived(proj_mate, mate_sems, (2,))

    def project(owner, slot, columns):
        return jnp.dot(
            gated[rows_of(owner), :], proj_own[:, columns], preferred_element_type=jnp.float32
        ) + jnp.dot(
            mate_gated[slot], proj_mate[:, columns], preferred_element_type=jnp.float32
        )

    arrived(mate_gated.at[0], mate_sems, (0,))
    for at in range(count):
        columns = slice(at * cols_out, (at + 1) * cols_out)
        part_send[at] = project(across, 0, columns).astype(jnp.bfloat16)
        send(part_send.at[at], part_recv.at[at], part_sems, (at,), to_y)
    pump(1)
    arrived(mate_gated.at[1], mate_sems, (1,))
    for at in range(count):
        columns = slice(at * cols_out, (at + 1) * cols_out)
        acc[:, columns] = project(me, 1, columns)
    pump(1)
    for name in ("residual", "outg", "ing"):
        loads[name].wait()
    for at in range(count):
        columns = slice(at * cols_out, (at + 1) * cols_out)
        arrived(part_recv.at[at], part_sems, (at,))
        acc[:, columns] = acc[:, columns] + part_recv[at].astype(jnp.float32)

    member = lambda parity, owner: parity * count + owner
    own = member(par, me)
    cut = block // 2
    for at in range(2):
        rows = slice(at * cut, (at + 1) * cut)
        mixed = acc[rows, :]
        scale = lax.rsqrt(jnp.mean(mixed * mixed, axis=-1, keepdims=True) + EPSILON)
        total = residual[rows, :].astype(jnp.float32) + mixed * scale * out_gain[...]
        total = total.astype(jnp.bfloat16)
        first_own[rows, :] = total
        long = total.astype(jnp.float32)
        scale = lax.rsqrt(jnp.mean(long * long, axis=-1, keepdims=True) + EPSILON)
        normed[own, rows, :] = (long * scale * in_gain[...]).astype(jnp.bfloat16)
        for slot, peer in ((0, to_mate), (1, to_y), (2, to_z)):
            spot = normed.at[own, rows, :]
            send(spot, spot, ag_sems, (slot, at), peer)
    for slot, owner in ((0, mate), (1, across), (2, corner)):
        columns = pl.ds(pl.multiple_of(owner * cols_out, cols_out), cols_out)
        send(first_own.at[:, columns], first_cols.at[me], first_sems, (slot,), {"tp": owner})
    columns = pl.ds(pl.multiple_of(me * cols_out, cols_out), cols_out)
    first_cols[me] = first_own[:, columns]
    x_weights(2)
    for i in (3, 2, 1):
        z_weights(2, i)

    facing = 1 - par
    came = {
        0: member(par, mate), 1: member(par, across), 2: member(facing, me),
        3: member(par, corner), 4: member(facing, mate), 5: member(facing, across),
        6: member(facing, corner),
    }

    def take(slot, onward):
        for at in range(2):
            spot = normed.at[came[slot], at * cut : (at + 1) * cut, :]
            arrived(spot, ag_sems, (slot, at))
            for further, peer in onward:
                send(spot, spot, ag_sems, (further, at), peer)

    pump(3)
    gathered(0)
    gathered(1)

    def mix(parity, at):
        base = pl.multiple_of(parity * count + 2 * at, 2)
        left_rows = normed[pl.ds(base, 2)].reshape(2 * block, width)
        gate = jnp.dot(left_rows, gate_w[...], preferred_element_type=jnp.float32)
        up = jnp.dot(left_rows, up_w[...], preferred_element_type=jnp.float32)
        gate = (gate / (1.0 + jnp.exp(-gate)) * up).astype(jnp.bfloat16)
        active[pl.ds(base, 2)] = gate.reshape(2, block, half)

    take(1, [(3, to_mate)])
    take(2, [(4, to_mate), (5, to_y)])
    take(0, [])
    mix(par, chip)
    take(5, [(6, to_mate)])
    take(3, [])
    mix(par, 1 - chip)
    pump(1)
    take(4, [])
    mix(facing, chip)
    pump(1)
    take(6, [])
    mix(facing, 1 - chip)
    pump(1)
    gathered(2)

    side = cols_out // 2

    def term(parity, owner):
        base = pl.multiple_of(parity * count, count)
        left_rows = active[pl.ds(base, count)].reshape(rows_all, half)
        return [
            jnp.dot(left_rows, down_w[2 * owner + at], preferred_element_type=jnp.float32)
            for at in range(2)
        ]

    targets = ((facing, 1 - chip), (par, 1 - chip), (facing, chip), (par, chip))

    def for_mate(at):
        parity, there = targets[at]
        for piece_at, value_at in enumerate(term(parity, 2 * there + 1 - core)):
            to_core[at, :, piece_at * side : (piece_at + 1) * side] = value_at.astype(
                jnp.bfloat16
            )
        send(to_core.at[at], from_core.at[at], core_sems, (at,), to_mate)

    def summed(at):
        parity, there = targets[at]
        low, top_part = term(parity, 2 * there + core)
        arrived(from_core.at[at], core_sems, (at,))
        return (
            low + from_core[at, :, :side].astype(jnp.float32),
            top_part + from_core[at, :, side:].astype(jnp.float32),
        )

    def pass_on(value_at, source, target, way, slot, peer):
        source[slot] = value_at.astype(jnp.bfloat16)
        send(source.at[slot], target.at[slot], link_sems, (way, slot), peer)

    for_mate(0)
    for_mate(1)
    low, top_part = summed(0)
    pass_on(low, y_send, y_recv, 0, 0, to_y)
    pass_on(top_part, z_send, z_recv, 1, 0, to_z)
    for_mate(2)
    low, top_part = summed(1)
    pass_on(low, y_send, y_recv, 0, 1, to_y)
    held[0] = top_part
    for_mate(3)
    low, top_part = summed(2)
    held[1] = low
    pass_on(top_part, z_send, z_recv, 1, 1, to_z)
    low, top_part = summed(3)
    kept[:, :side] = low
    kept[:, side:] = top_part
    arrived(y_recv.at[0], link_sems, (0, 0))
    pass_on(held[1] + y_recv[0].astype(jnp.float32), z_send, z_recv, 1, 2, to_z)
    arrived(z_recv.at[0], link_sems, (1, 0))
    pass_on(held[0] + z_recv[0].astype(jnp.float32), y_send, y_recv, 0, 2, to_y)
    for slot, owner in ((0, mate), (1, across), (2, corner)):
        arrived(first_cols.at[owner], first_sems, (slot,))
    base_rows = first_cols[...].reshape(rows_all, cols_out).astype(jnp.float32)
    arrived(y_recv.at[1], link_sems, (0, 1))
    arrived(z_recv.at[1], link_sems, (1, 1))
    kept[:, :side] = kept[:, :side] + y_recv[1].astype(jnp.float32)
    kept[:, side:] = kept[:, side:] + z_recv[1].astype(jnp.float32)
    arrived(z_recv.at[2], link_sems, (1, 2))
    out_ref[:, :side] = (
        base_rows[:, :side] + 0.5 * (kept[:, :side] + z_recv[2].astype(jnp.float32))
    ).astype(jnp.bfloat16)
    arrived(y_recv.at[2], link_sems, (0, 2))
    out_ref[:, side:] = (
        base_rows[:, side:] + 0.5 * (kept[:, side:] + y_recv[2].astype(jnp.float32))
    ).astype(jnp.bfloat16)
    for copy in sent:
        copy.wait_send()
    for step in range(1, depth):

        @pl.when(row + step < depth)
        def _():
            for copy in plane_copies(step):
                copy.wait_send()


def paired(logs, cell_inputs, rows_inputs, weights):
    ranks, count = lax.axis_size("sp"), lax.axis_size("tp")
    heads = logs[0].shape[0]
    residual, out_gain, in_gain = rows_inputs
    projection, gate_weight, up_weight, down_weight = weights
    rows, width = residual.shape
    inner = projection.shape[0]
    half = gate_weight.shape[1] // 2
    cols = width // count
    block, side, depth = rows // count, cols // 2, ranks // 2
    dma = pltpu.SemaphoreType.DMA

    def low(*shape):
        return pltpu.VMEM(shape, jnp.bfloat16)

    def full(*shape):
        return pltpu.VMEM(shape, jnp.float32)

    like = lambda array: pltpu.VMEM(array.shape, array.dtype)
    members = 2 * count
    operands = (*logs, *cell_inputs, residual, out_gain, in_gain, *weights)
    return pl.pallas_call(
        functools.partial(pair_kernel, ranks, count, heads),
        out_shape=jax.ShapeDtypeStruct((rows, cols), jnp.bfloat16),
        in_specs=[ANY] * len(operands),
        out_specs=VMEM,
        scratch_shapes=[
            *(like(array) for array in (*logs, *cell_inputs)),
            low(block, width), full(1, width), full(1, width),
            low(inner, width), low(inner, width),
            low(width, half), low(width, half), low(ranks, half, down_weight.shape[1]),
            full(heads, rows), full(rows, 128),
            full(heads, DQK, DV), low(heads, DQK, DV), full(heads, 8, DQK),
            low(DQK, DV), full(8, DQK),
            full(DQK, DV), full(8, DQK),
            low(DQK, DV), full(8, DQK),
            low(depth - 1, DQK, DV), full(depth - 1, 8, DQK),
            full(DQK, DV), full(8, DQK),
            low(DQK, DV), full(8, DQK),
            low(heads, DQK, DV), full(heads, 8, DQK),
            full(rows, inner), low(rows, inner), low(2, block, inner),
            low(count, block, cols), low(count, block, cols), full(block, width),
            low(block, width), low(count, block, cols),
            low(members, block, width), low(members, block, half),
            low(4, rows, cols), low(4, rows, cols),
            low(3, rows, side), low(3, rows, side), low(3, rows, side), low(3, rows, side),
            full(2, rows, side), full(rows, cols),
            dma((15,)), dma((2, 3, 2, depth)), dma((2, 4)), dma((2, 2, depth - 1)), dma((2, 3)),
            dma((2, count)), dma((2, 7, 2)), dma((2, 3)), dma((2, 4)), dma((2, 2, 3)),
        ],
        compiler_params=pltpu.CompilerParams(
            collective_id=0, has_side_effects=True, vmem_limit_bytes=VMEM_BYTES
        ),
        name="layer",
    )(*operands)


def body(
    residual,
    query_matrix,
    key_matrix,
    value_matrix,
    output_gate_logit,
    input_gate_log,
    forget_gate_logit,
    extra_head_decay,
    head_norm_gain,
    projection,
    cell_output_gain,
    mixer_input_gain,
    mixer_gate_weight,
    mixer_up_weight,
    mixer_down_weight,
):
    heads_here = input_gate_log.shape[1]
    if (lax.axis_size("sp"), lax.axis_size("tp"), heads_here) == (8, 4, 2):
        return paired(
            (forget_gate_logit.T, extra_head_decay.T, input_gate_log.T),
            (query_matrix, key_matrix, value_matrix, output_gate_logit, head_norm_gain[None]),
            (residual, cell_output_gain[None], mixer_input_gain[None]),
            (projection, mixer_gate_weight, mixer_up_weight, mixer_down_weight),
        )
    key_low = heads_first(key_matrix, heads_here, DQK)
    value_low = heads_first(value_matrix, heads_here, DV)
    keyed = key_low.astype(jnp.float32)
    valued = value_low.astype(jnp.float32)
    in_logs = input_gate_log.T
    running_log_total = jnp.cumsum(
        (jax.nn.log_sigmoid(forget_gate_logit) + extra_head_decay).T, axis=-1
    )
    zero_memory = jnp.zeros((heads_here, DV, DQK), jnp.float32)
    zero_normalizer = jnp.zeros((heads_here, DQK), jnp.float32)
    lowest = jnp.full((heads_here,), LOWEST_LOG, jnp.float32)
    local_memory, local_normalizer, local_max = fold_state(
        keyed, valued, in_logs, running_log_total, zero_memory, zero_normalizer, lowest
    )
    return layer(
        (running_log_total[:, -1], local_memory, local_normalizer, local_max),
        (running_log_total, in_logs),
        (query_matrix, key_matrix, value_matrix, output_gate_logit, head_norm_gain[None]),
        residual,
        (cell_output_gain[None], mixer_input_gain[None]),
        (projection, mixer_gate_weight, mixer_up_weight, mixer_down_weight),
    )


def solution(mesh):
    return jax.shard_map(
        body,
        mesh=mesh,
        in_specs=(
            P("sp", None),
            P("sp", "tp"),
            P("sp", "tp"),
            P("sp", "tp"),
            P("sp", "tp"),
            P("sp", "tp"),
            P("sp", "tp"),
            P("sp", "tp"),
            P("tp"),
            P("tp", None),
            P(),
            P(),
            P("sp", "tp"),
            P("sp", "tp"),
            P("tp", "sp"),
        ),
        out_specs=P("sp", "tp"),
        check_vma=False,
    )
```

```python
import functools

import jax
import jax.numpy as jnp
from jax import lax
from jax.experimental import pallas as pl
from jax.experimental.pallas import tpu as pltpu
from jax.sharding import PartitionSpec as P

DQK = 128
DV = 256
MESH = pl.DeviceIdType.MESH
VMEM = pl.BlockSpec(memory_space=pltpu.VMEM)
ANY = pl.BlockSpec(memory_space=pl.ANY)
VMEM_BYTES = 62 * 1024 * 1024

HIGHEST = lax.Precision.HIGHEST
EPSILON = 1e-06
LOWEST_LOG = -1e30


def heads_first(array, heads, width):
    return array.reshape(array.shape[0], heads, width).transpose(1, 0, 2)


def fold_state(keyed, valued, in_logs, running_log_total, memory, normalizer, stabilizer):
    last = running_log_total[:, -1]
    lifted = last[:, None] - running_log_total + in_logs
    new_max = jnp.maximum(last + stabilizer, jnp.max(lifted, axis=-1))
    weights = jnp.exp(lifted - new_max[:, None])
    retained = jnp.exp(last + stabilizer - new_max)
    memory = retained[:, None, None] * memory + jnp.einsum(
        "hsv,hsd->hvd", weights[:, :, None] * valued, keyed, precision=HIGHEST
    )
    normalizer = retained[:, None] * normalizer + jnp.einsum(
        "hs,hsd->hd", weights, keyed, precision=HIGHEST
    )
    return (memory, normalizer, new_max)


def copy_to(source, target, sems, slot, peer):
    return pltpu.make_async_remote_copy(
        source, target, sems.at[(0, *slot)], sems.at[(1, *slot)], device_id=peer, device_id_type=MESH
    )


def layer_kernel(
    ranks, count, heads, memory_ref, aux_ref, cum_row, in_row, cum_col, query_ref,
    key_ref, value_ref, ogate_ref, head_gain, residual_ref, out_gain, in_gain, projection_ref,
    gate_ref, up_ref, down_ref, out_ref, slots, aux_slots, memory, aux, gate_w, up_w, down_w,
    weight, gated, blocks, normed, first, active, to_core, from_core, to_chip, from_chip,
    state_sems, aux_sems, local_sems, proj_sems, gated_sems, sum_sems,
):
    sp, me = lax.axis_index("sp"), lax.axis_index("tp")
    core = lax.rem(me, 2)
    mate = me + 1 - 2 * core
    chips = count // 2
    rows_all, width = residual_ref.shape
    cols = out_ref.shape[1]
    inner = value_ref.shape[1]

    barrier = pltpu.get_barrier_semaphore()
    for axis, size, at in (("sp", ranks, sp), ("tp", count, me)):
        for step in range(1, size):
            pl.semaphore_signal(
                barrier, inc=1, device_id={axis: lax.rem(at + step, size)}, device_id_type=MESH
            )
    pl.semaphore_wait(barrier, ranks + count - 2)

    def state_copies(step):
        peer = {"sp": lax.rem(sp + step, ranks)}
        return (
            copy_to(memory_ref, slots.at[step - 1], state_sems, (step - 1,), peer),
            copy_to(aux_ref, aux_slots.at[step - 1], aux_sems, (step - 1,), peer),
        )

    for step in range(1, ranks):

        @pl.when(sp + step < ranks)
        def _():
            for copy in state_copies(step):
                copy.start()

    def spread(source, whole, sems):
        sent = [copy_to(source, whole.at[me], sems, (0,), {"tp": mate})]
        for step in range(1, chips):
            peer = {"tp": lax.rem(me + 2 * step, count)}
            sent.append(copy_to(source, whole.at[me], sems, (2 * step,), peer))
        for copy in sent:
            copy.start()
        return sent

    def relay(whole, sems):
        sent = []
        for step in range(1, chips):
            owner = lax.rem(me - 2 * step + count, count)
            block = whole.at[owner]
            copy_to(block, block, sems, (2 * step,), {"tp": mate}).wait_recv()
            sent.append(copy_to(block, block, sems, (2 * step - 1,), {"tp": mate}))
            sent[-1].start()
        return sent

    def collect(whole, sems):
        for step in range(chips):
            owner = lax.rem(mate - 2 * step + count, count)
            block = whole.at[owner]
            slot = 0 if step == 0 else 2 * step - 1
            copy_to(block, block, sems, (slot,), {"tp": mate}).wait_recv()

    for ref, whole, at in ((gate_ref, gate_w, 0), (up_ref, up_w, 1)):
        pltpu.make_async_copy(ref, whole, local_sems.at[at]).start()
    pltpu.make_async_copy(down_ref, down_w.at[0], local_sems.at[2]).start()
    own_weight = pltpu.make_async_copy(projection_ref, weight.at[me], local_sems.at[4])
    own_weight.start()
    sent = spread(projection_ref, weight, proj_sems)

    memory[...] = jnp.zeros_like(memory)
    aux[...] = jnp.zeros_like(aux)
    aux[heads : 2 * heads, :] = jnp.full((heads, DQK), LOWEST_LOG, jnp.float32)
    for step in range(ranks - 1, 0, -1):

        @pl.when(sp >= step)
        def _():
            for copy in state_copies(step):
                copy.wait_recv()
            late = aux_slots[step - 1]
            for head in range(heads):
                rows = pl.ds(head * DV, DV)
                early_max = aux[heads + head : heads + head + 1, :]
                late_max = late[heads + head : heads + head + 1, :]
                late_decay = late[2 * heads + head : 2 * heads + head + 1, :]
                joined = jnp.maximum(late_decay + early_max, late_max)
                before = jnp.exp(late_decay + early_max - joined)
                after = jnp.exp(late_max - joined)
                memory[rows, :] = before * memory[rows, :] + after * slots[
                    step - 1, rows, :
                ].astype(jnp.float32)
                aux[head : head + 1, :] = (
                    before * aux[head : head + 1, :] + after * late[head : head + 1, :]
                )
                aux[heads + head : heads + head + 1, :] = joined
                aux[2 * heads + head : 2 * heads + head + 1, :] = (
                    aux[2 * heads + head : 2 * heads + head + 1, :] + late_decay
                )

    tile = rows_all // 3
    for head in range(heads):
        prior_max = aux[heads + head : heads + head + 1, :]
        start_max = jnp.maximum(aux[2 * heads + head : 2 * heads + head + 1, :], prior_max)
        lift = jnp.exp(prior_max - start_max) * DQK ** (-0.5)
        memory[head * DV : (head + 1) * DV, :] = memory[head * DV : (head + 1) * DV, :] * lift
        aux[head : head + 1, :] = aux[head : head + 1, :] * lift
        aux[2 * heads + head : 2 * heads + head + 1, :] = start_max

    def read(at, unused):
        start = pl.multiple_of(at * tile, tile)
        rows = pl.ds(start, tile)
        causal = start + lax.broadcasted_iota(
            jnp.int32, (tile, rows_all), 0
        ) >= lax.broadcasted_iota(jnp.int32, (tile, rows_all), 1)
        for head in range(heads):
            keys = slice(head * DQK, (head + 1) * DQK)
            values = slice(head * DV, (head + 1) * DV)
            query = query_ref[rows, keys]
            total = cum_col[rows, head : head + 1]
            spread_log = total - cum_row[head : head + 1, :] + in_row[head : head + 1, :]
            spread_log = jnp.where(causal, spread_log, -jnp.inf)
            carried = total + aux[2 * heads + head : 2 * heads + head + 1, :1]
            running = jnp.maximum(carried, jnp.max(spread_log, axis=-1, keepdims=True))
            scores = lax.dot_general(
                query, key_ref[:, keys], (((1,), (1,)), ((), ())),
                preferred_element_type=jnp.float32,
            ) * DQK ** (-0.5)
            weights = jnp.exp(spread_log - running) * scores
            scaled = jnp.exp(carried - running)
            wide = query.astype(jnp.float32)
            numerator = jnp.dot(
                weights.astype(jnp.bfloat16), value_ref[:, values],
                preferred_element_type=jnp.float32,
            ) + scaled * lax.dot_general(
                wide, memory[values, :], (((1,), (1,)), ((), ())), precision=HIGHEST,
                preferred_element_type=jnp.float32,
            )
            denominator = jnp.sum(weights, axis=-1, keepdims=True) + scaled * jnp.sum(
                wide * aux[head : head + 1, :], axis=-1, keepdims=True
            )
            cell = numerator / jnp.maximum(jnp.abs(denominator), jnp.exp(-running))
            centered = cell - jnp.mean(cell, axis=-1, keepdims=True)
            cell = centered * lax.rsqrt(
                jnp.mean(centered * centered, axis=-1, keepdims=True) + EPSILON
            )
            cell = cell * head_gain[:, values]
            gate = ogate_ref[rows, values].astype(jnp.float32)
            gated[rows, values] = (cell * jax.nn.sigmoid(gate)).astype(jnp.bfloat16)
        return unused

    lax.fori_loop(0, 3, read, 0)
    sent += spread(gated, blocks, gated_sems)
    blocks[me] = gated[...]
    sent += relay(weight, proj_sems)
    sent += relay(blocks, gated_sems)
    collect(weight, proj_sems)
    own_weight.wait()
    collect(blocks, gated_sems)

    def turn(at, unused):
        rows = pl.ds(pl.multiple_of(at * tile, tile), tile)
        mixed = jnp.zeros((tile, width), jnp.float32)
        for block in range(count):
            mixed = mixed + jnp.dot(
                blocks[block, rows, :], weight[block], preferred_element_type=jnp.float32
            )
        scale = lax.rsqrt(jnp.mean(mixed * mixed, axis=-1, keepdims=True) + EPSILON)
        total = residual_ref[rows, :].astype(jnp.float32) + mixed * scale * out_gain[...]
        total = total.astype(jnp.bfloat16)
        first[rows, :] = total
        wide = total.astype(jnp.float32)
        scale = lax.rsqrt(jnp.mean(wide * wide, axis=-1, keepdims=True) + EPSILON)
        normed[rows, :] = (wide * scale * in_gain[...]).astype(jnp.bfloat16)
        return unused

    lax.fori_loop(0, 3, turn, 0)

    for ref, whole, at in ((gate_ref, gate_w, 0), (up_ref, up_w, 1)):
        pltpu.make_async_copy(ref, whole, local_sems.at[at]).wait()

    def mix(at, unused):
        rows = pl.ds(pl.multiple_of(at * tile, tile), tile)
        left = normed[rows, :]
        gate = jnp.dot(left, gate_w[...], preferred_element_type=jnp.float32)
        up = jnp.dot(left, up_w[...], preferred_element_type=jnp.float32)
        active[rows, :] = (gate / (1.0 + jnp.exp(-gate)) * up).astype(jnp.bfloat16)
        return unused

    lax.fori_loop(0, 3, mix, 0)
    pltpu.make_async_copy(down_ref, down_w.at[0], local_sems.at[2]).wait()

    def term(target):
        start = pl.multiple_of(target * cols, cols)
        return jnp.dot(
            active[...], down_w[0, :, pl.ds(start, cols)], preferred_element_type=jnp.float32
        )

    def send(source, target, kind, at, peer):
        return copy_to(source.at[at], target.at[at], sum_sems.at[kind], (at,), {"tp": peer})

    copies = []
    for step in range(1, chips):
        away = lax.rem(me + 2 * step, count)
        to_core[step] = term(away + 1 - 2 * core).astype(jnp.bfloat16)
        hop = send(to_core, from_core, 0, step, mate)
        hop.start()
        mine = term(away)
        hop.wait_recv()
        to_chip[step] = (mine + from_core[step].astype(jnp.float32)).astype(jnp.bfloat16)
        far = send(to_chip, from_chip, 1, step, away)
        far.start()
        copies += [hop, far]
    to_core[0] = term(mate).astype(jnp.bfloat16)
    hop = send(to_core, from_core, 0, 0, mate)
    hop.start()
    result = term(me)
    hop.wait_recv()
    result = result + from_core[0].astype(jnp.float32)
    for far in copies[1::2]:
        far.wait_recv()
    for step in range(1, chips):
        result = result + from_chip[step].astype(jnp.float32)
    own_first = first[:, pl.ds(pl.multiple_of(me * cols, cols), cols)]
    out_ref[...] = (own_first.astype(jnp.float32) + 0.5 * result).astype(jnp.bfloat16)
    for copy in copies + [hop] + sent:
        copy.wait_send()
    for step in range(1, ranks):

        @pl.when(sp + step < ranks)
        def _():
            for copy in state_copies(step):
                copy.wait_send()


def layer(states, logs, cell_inputs, residual, gains, weights):
    decay, memory, normalizer, maximum = states
    running_log_total, in_logs = logs
    ranks, count = lax.axis_size("sp"), lax.axis_size("tp")
    heads = decay.shape[0]
    rows, width = residual.shape
    projection, gate_weight, up_weight, down_weight = weights
    hidden = gate_weight.shape[1]
    inner = projection.shape[0]
    gate_weight = lax.all_gather(gate_weight, "sp", axis=0, tiled=True)
    up_weight = lax.all_gather(up_weight, "sp", axis=0, tiled=True)
    down_weight = lax.all_gather(down_weight, "sp", axis=1, tiled=True)
    down_shape = (1, hidden, width)
    fill = lambda row: jnp.broadcast_to(row[:, None], (heads, DQK))
    aux = jnp.concatenate([normalizer, fill(maximum), fill(decay)])
    height = -(-3 * heads // 8) * 8
    aux = jnp.pad(aux, ((0, height - 3 * heads), (0, 0)))
    low = memory.reshape(heads * DV, DQK).astype(jnp.bfloat16)
    chips, cols = count // 2, width // count
    buffer = pltpu.VMEM((chips, rows, cols), jnp.bfloat16)
    dma = pltpu.SemaphoreType.DMA
    return pl.pallas_call(
        functools.partial(layer_kernel, ranks, count, heads),
        out_shape=jax.ShapeDtypeStruct((rows, cols), jnp.bfloat16),
        in_specs=[VMEM] * 13 + [ANY] * 4,
        out_specs=VMEM,
        scratch_shapes=[
            pltpu.VMEM((ranks - 1, heads * DV, DQK), jnp.bfloat16),
            pltpu.VMEM((ranks - 1, height, DQK), jnp.float32),
            pltpu.VMEM((heads * DV, DQK), jnp.float32),
            pltpu.VMEM((height, DQK), jnp.float32),
            pltpu.VMEM((width, hidden), jnp.bfloat16),
            pltpu.VMEM((width, hidden), jnp.bfloat16),
            pltpu.VMEM(down_shape, jnp.bfloat16),
            pltpu.VMEM((count, inner, width), jnp.bfloat16),
            pltpu.VMEM((rows, inner), jnp.bfloat16),
            pltpu.VMEM((count, rows, inner), jnp.bfloat16),
            pltpu.VMEM((rows, width), jnp.bfloat16),
            pltpu.VMEM((rows, width), jnp.bfloat16),
            pltpu.VMEM((rows, hidden), jnp.bfloat16),
            buffer, buffer, buffer, buffer,
            dma((2, ranks - 1)),
            dma((2, ranks - 1)),
            dma((5,)),
            dma((2, count)),
            dma((2, count)),
            dma((2, 2, chips)),
        ],
        compiler_params=pltpu.CompilerParams(
            collective_id=0, has_side_effects=True, vmem_limit_bytes=VMEM_BYTES
        ),
        name="layer",
    )(
        low, aux, running_log_total, in_logs, running_log_total.T, *cell_inputs, residual,
        *gains, projection, gate_weight, up_weight, down_weight,
    )


def pair_kernel(
    ranks, count, heads, forget_hbm, extra_hbm, in_hbm, query_hbm, key_hbm, value_hbm, ogate_hbm,
    head_gain_hbm, residual_hbm, out_gain_hbm, in_gain_hbm, projection_hbm, gate_hbm, up_hbm,
    down_hbm, out_ref, forget, extra, in_row, query, key, value, ogate, head_gain, residual,
    out_gain, in_gain, proj_own, proj_mate, gate_w, up_w, down_w, cum_row, cols, own_mem, mem_send,
    aux, x_mem, x_aux, e_mem, e_aux, t_mem, t_aux, z_mem, z_aux, p_mem, p_aux, q_mem, q_aux,
    final_mem, final_aux, local, gated, mate_gated, part_send, part_recv, acc, first_own,
    first_cols, normed, active, to_core, from_core, y_send, y_recv, z_send, z_recv, held, kept,
    local_sems, w_sems, state_sems, line_sems, mate_sems, part_sems, ag_sems, first_sems,
    core_sems, link_sems,
):
    sp, me = lax.axis_index("sp"), lax.axis_index("tp")
    row, col = sp // 2, lax.rem(sp, 2)
    depth = ranks // 2
    par = lax.rem(row, 2)
    core = lax.rem(me, 2)
    chip = me // 2
    mate = me + 1 - 2 * core
    across = lax.rem(me + 2, count)
    corner = lax.rem(mate + 2, count)
    rows_all, width = out_ref.shape[0], out_gain.shape[1]
    cols_out = out_ref.shape[1]
    block = rows_all // count
    half = gate_w.shape[1]
    high = gate_hbm.shape[0]
    others = {1: row + 1 - 2 * par, 2: lax.rem(row + 2, depth), 3: depth - 1 - row}
    inner_row = jnp.logical_or(row == 1, row == 2)
    to_x = {"sp": row * 2 + 1 - col}
    to_z = {"sp": others[1] * 2 + col}
    to_mate, to_y = {"tp": mate}, {"tp": across}
    sent = []

    barrier = pltpu.get_barrier_semaphore()
    greeted = [{"sp": others[i] * 2 + col} for i in (1, 2, 3)]
    greeted += [to_x, to_mate, to_y, {"tp": corner}]
    for peer in greeted:
        pl.semaphore_signal(barrier, inc=1, device_id=peer, device_id_type=MESH)

    loads = {}

    def load(name, source, target):
        loads[name] = pltpu.make_async_copy(source, target, local_sems.at[len(loads)])
        loads[name].start()

    load("forget", forget_hbm, forget)
    load("extra", extra_hbm, extra)
    load("in", in_hbm, in_row)
    load("key", key_hbm, key)
    load("value", value_hbm, value)
    load("query", query_hbm, query)
    load("ogate", ogate_hbm, ogate)
    load("head", head_gain_hbm, head_gain)
    load("proj", projection_hbm, proj_own)
    own_rows = pl.ds(pl.multiple_of(me * block, block), block)
    load("residual", residual_hbm.at[own_rows, :], residual)
    load("outg", out_gain_hbm, out_gain)
    load("ing", in_gain_hbm, in_gain)

    def piece(kind, parity):
        at = pl.ds(pl.multiple_of(parity * half, half), half)
        if kind == 2:
            return down_hbm.at[at, :]
        return (gate_hbm, up_hbm)[kind].at[:, at]

    def place(kind, owner):
        if kind == 2:
            return down_w.at[owner]
        at = pl.ds(pl.multiple_of(owner * high, high), high)
        return (gate_w, up_w)[kind].at[at, :]

    for kind in range(3):
        load(kind, piece(kind, par), place(kind, sp))

    pl.semaphore_wait(barrier, len(greeted))

    def send(source, target, sems, slot, peer):
        copy = copy_to(source, target, sems, slot, peer)
        copy.start()
        sent.append(copy)

    def arrived(target, sems, slot):
        copy_to(target, target, sems, slot, to_mate).wait_recv()

    def z_copy(kind, i):
        there = others[i]
        return copy_to(
            piece(kind, lax.rem(there, 2)), place(kind, sp), w_sems, (kind, 0, i),
            {"sp": there * 2 + col},
        )

    def z_weights(condition, *pieces):
        @pl.when(condition)
        def _():
            for kind, i in pieces:
                z_copy(kind, i).start()

    def x_weights(kind):
        send(piece(kind, par), place(kind, sp), w_sems, (kind, 1, 0), to_x)

    relays = [(0, 1), (1, 1), (0, 3), (0, 2), (1, 3), (1, 2), (2, "soon"), (2, "late"), (2, 2)]
    steps = {"soon": jnp.where(inner_row, 3, 1), "late": jnp.where(inner_row, 1, 3)}
    others |= {
        "soon": jnp.where(inner_row, others[3], others[1]),
        "late": jnp.where(inner_row, others[1], others[3]),
    }

    def pump(number):
        for _ in range(number):
            kind, i = relays.pop(0)
            spot = place(kind, others[i] * 2 + col)
            step = steps.get(i, i)
            arrived(spot, w_sems, (kind, 0, step))
            send(spot, spot, w_sems, (kind, 1, step), to_x)

    def gathered(kind):
        for i in range(depth):
            there = row if i == 0 else others[i]
            arrived(place(kind, there * 2 + 1 - col), w_sems, (kind, 1, i))

    odd, lower = par == 1, row < depth // 2
    z_weights(row >= 0, (0, 1))
    z_weights(row == 1, (0, 3))
    z_weights(odd, (1, 1))
    z_weights(jnp.logical_not(lower), (0, 3), (0, 2), (1, 3), (1, 2))
    z_weights(row == 1, (2, 1))
    z_weights(row == 2, (2, 3))
    send(projection_hbm, proj_mate, mate_sems, (2,), to_mate)

    for name in ("forget", "extra", "in"):
        loads[name].wait()
    logit = forget[...]
    decay = jnp.minimum(logit, 0.0) - jnp.log1p(jnp.exp(-jnp.abs(logit))) + extra[...]
    lane = lax.broadcasted_iota(jnp.int32, decay.shape, 1)
    shift = 1
    while shift < rows_all:
        decay = decay + jnp.where(lane >= shift, pltpu.roll(decay, shift, 1), 0.0)
        shift *= 2
    cum_row[...] = decay
    last = decay[:, rows_all - 1 : rows_all]
    lifted = last - decay + in_row[...]
    top = jnp.max(lifted, axis=-1, keepdims=True)
    lifted = jnp.exp(lifted - top)
    eye = lax.broadcasted_iota(jnp.int32, (128, 128), 0) == lax.broadcasted_iota(
        jnp.int32, (128, 128), 1
    )

    def to_column(line, at):
        for start in range(0, rows_all, 128):
            spread = jnp.broadcast_to(line[:, start : start + 128], (128, 128))
            cols[start : start + 128, at : at + 1] = jnp.sum(
                jnp.where(eye, spread, 0.0), axis=-1, keepdims=True
            )

    for head in range(heads):
        to_column(decay[head : head + 1, :], head)
        to_column(lifted[head : head + 1, :], heads + head)
    loads["key"].wait()
    loads["value"].wait()
    for head in range(heads):
        keys = slice(head * DQK, (head + 1) * DQK)
        values = slice(head * DV, (head + 1) * DV)
        share = cols[:, heads + head : heads + head + 1]
        heavy = (share * value[:, values].astype(jnp.float32)).astype(jnp.bfloat16)
        state = lax.dot_general(
            key[:, keys], heavy, (((0,), (0,)), ((), ())), preferred_element_type=jnp.float32
        )
        own_mem[head] = state
        mem_send[head] = state.astype(jnp.bfloat16)
        aux[head] = jnp.zeros((8, DQK), jnp.float32)
        aux[head, 0:1, :] = jnp.sum(
            share * key[:, keys].astype(jnp.float32), axis=0, keepdims=True
        )
        aux[head, 1:2, :] = jnp.broadcast_to(top[head : head + 1, :], (1, DQK))
        aux[head, 2:3, :] = jnp.broadcast_to(last[head : head + 1, :], (1, DQK))
    send(mem_send.at[1 - col], x_mem, state_sems, (0,), to_x)
    send(aux.at[1 - col], x_aux, state_sems, (1,), to_x)
    x_weights(0)

    tile = rows_all // 3
    loads["query"].wait()

    def nearby(head, at):
        start, reach = at * tile, (at + 1) * tile
        keys = slice(head * DQK, (head + 1) * DQK)
        values = slice(head * DV, (head + 1) * DV)
        rows = slice(start, reach)
        causal = start + lax.broadcasted_iota(
            jnp.int32, (tile, reach), 0
        ) >= lax.broadcasted_iota(jnp.int32, (tile, reach), 1)
        total = cols[rows, head : head + 1]
        spread_log = total - cum_row[head : head + 1, :reach] + in_row[head : head + 1, :reach]
        spread_log = jnp.where(causal, spread_log, -jnp.inf)
        running = jnp.max(spread_log, axis=-1, keepdims=True)
        scores = lax.dot_general(
            query[rows, keys], key[:reach, keys], (((1,), (1,)), ((), ())),
            preferred_element_type=jnp.float32,
        ) * DQK ** (-0.5)
        weights = jnp.exp(spread_log - running) * scores
        local[rows, values] = jnp.dot(
            weights.astype(jnp.bfloat16), value[:reach, values],
            preferred_element_type=jnp.float32,
        )
        cols[rows, 2 * heads + head : 2 * heads + head + 1] = running
        cols[rows, 3 * heads + head : 3 * heads + head + 1] = jnp.sum(
            weights, axis=-1, keepdims=True
        )

    nearby(0, 0)
    nearby(1, 0)
    nearby(0, 1)

    def parts(ref):
        return ref[0:1, :], ref[1:2, :], ref[2:3, :]

    def join(early_mem, early, late_mem, late):
        joined = jnp.maximum(late[2] + early[1], late[1])
        before = jnp.exp(late[2] + early[1] - joined)
        after = jnp.exp(late[1] - joined)
        memory = before[:, :1] * early_mem + after[:, :1] * late_mem
        return memory, (before * early[0] + after * late[0], joined, early[2] + late[2])

    def keep(ref, values):
        ref[...] = jnp.zeros(ref.shape, jnp.float32)
        for at, entry in enumerate(values):
            ref[at : at + 1, :] = entry

    left = col == 0
    arrived(x_mem, state_sems, (0,))
    arrived(x_aux, state_sems, (1,))
    mine, theirs = own_mem[col], x_mem[...].astype(jnp.float32)
    mine_aux = tuple(aux[col, at : at + 1, :] for at in range(3))
    theirs_aux = parts(x_aux)
    pick = lambda one, two: jnp.where(left, one, two)
    early_mem, late_mem = pick(mine, theirs), pick(theirs, mine)
    early_aux = tuple(pick(one, two) for one, two in zip(mine_aux, theirs_aux))
    late_aux = tuple(pick(two, one) for one, two in zip(mine_aux, theirs_aux))
    e_mem[...] = early_mem
    keep(e_aux, early_aux)
    both, both_aux = join(early_mem, early_aux, late_mem, late_aux)
    t_mem[...] = both.astype(jnp.bfloat16)
    keep(t_aux, both_aux)

    def plane_copies(step):
        peer = {"sp": lax.rem(sp + 2 * step, ranks)}
        return (
            copy_to(t_mem, z_mem.at[step - 1], line_sems, (0, step - 1), peer),
            copy_to(t_aux, z_aux.at[step - 1], line_sems, (1, step - 1), peer),
        )

    for step in range(1, depth):

        @pl.when(row + step < depth)
        def _():
            for copy in plane_copies(step):
                copy.start()

    z_weights(par == 0, (1, 1))
    z_weights(row == 0, (0, 3))
    z_weights(lower, (0, 2), (1, 3), (1, 2))
    z_weights(row == 2, (2, 1))
    z_weights(row == 1, (2, 3))
    nearby(1, 1)
    nearby(0, 2)
    nearby(1, 2)

    p_mem[...] = jnp.zeros(p_mem.shape, jnp.float32)
    zero = jnp.zeros((1, DQK), jnp.float32)
    keep(p_aux, (zero, jnp.full((1, DQK), LOWEST_LOG, jnp.float32), zero))
    for step in range(depth - 1, 0, -1):

        @pl.when(row >= step)
        def _():
            for copy in plane_copies(step):
                copy.wait_recv()
            memory, rest = join(
                p_mem[...], parts(p_aux), z_mem[step - 1].astype(jnp.float32),
                parts(z_aux.at[step - 1]),
            )
            p_mem[...] = memory
            keep(p_aux, rest)

    prior, prior_aux = p_mem[...], parts(p_aux)
    more, more_aux = join(prior, prior_aux, e_mem[...], parts(e_aux))
    q_mem[...] = pick(more, prior).astype(jnp.bfloat16)
    keep(q_aux, tuple(pick(one, two) for one, two in zip(more_aux, prior_aux)))
    send(q_mem, final_mem.at[col], state_sems, (2,), to_x)
    send(q_aux, final_aux.at[col], state_sems, (3,), to_x)
    x_weights(1)
    x_weights(2)
    final_mem[col] = pick(prior, more).astype(jnp.bfloat16)
    keep(final_aux.at[col], tuple(pick(two, one) for one, two in zip(more_aux, prior_aux)))
    loads["ogate"].wait()
    loads["head"].wait()
    arrived(final_mem.at[1 - col], state_sems, (2,))
    arrived(final_aux.at[1 - col], state_sems, (3,))

    for head in range(heads):
        keys = slice(head * DQK, (head + 1) * DQK)
        values = slice(head * DV, (head + 1) * DV)
        prior_max = final_aux[head, 1:2, :]
        start_max = jnp.maximum(final_aux[head, 2:3, :], prior_max)
        lift = (jnp.exp(prior_max - start_max) * DQK ** (-0.5))[:, :1]
        start_max = start_max[:, :1]
        for at in range(3):
            rows = slice(at * tile, (at + 1) * tile)
            question = query[rows, keys]
            found = cols[rows, 2 * heads + head : 2 * heads + head + 1]
            carried = cols[rows, head : head + 1] + start_max
            running = jnp.maximum(carried, found)
            inside = jnp.exp(found - running)
            scaled = jnp.exp(carried - running) * lift
            numerator = inside * local[rows, values] + scaled * jnp.dot(
                question, final_mem[head], preferred_element_type=jnp.float32
            )
            denominator = inside * cols[
                rows, 3 * heads + head : 3 * heads + head + 1
            ] + scaled * jnp.sum(
                question.astype(jnp.float32) * final_aux[head, 0:1, :], axis=-1, keepdims=True
            )
            cell = numerator / jnp.maximum(jnp.abs(denominator), jnp.exp(-running))
            centered = cell - jnp.mean(cell, axis=-1, keepdims=True)
            cell = centered * lax.rsqrt(
                jnp.mean(centered * centered, axis=-1, keepdims=True) + EPSILON
            )
            gate = ogate[rows, values].astype(jnp.float32)
            gated[rows, values] = (
                cell * head_gain[:, values] * jax.nn.sigmoid(gate)
            ).astype(jnp.bfloat16)

    def rows_of(owner):
        return pl.ds(pl.multiple_of(owner * block, block), block)

    send(gated.at[rows_of(corner), :], mate_gated.at[0], mate_sems, (0,), to_mate)
    send(gated.at[rows_of(mate), :], mate_gated.at[1], mate_sems, (1,), to_mate)
    loads["proj"].wait()
    arrived(proj_mate, mate_sems, (2,))

    def project(owner, slot, columns):
        return jnp.dot(
            gated[rows_of(owner), :], proj_own[:, columns], preferred_element_type=jnp.float32
        ) + jnp.dot(
            mate_gated[slot], proj_mate[:, columns], preferred_element_type=jnp.float32
        )

    arrived(mate_gated.at[0], mate_sems, (0,))
    for at in range(count):
        columns = slice(at * cols_out, (at + 1) * cols_out)
        part_send[at] = project(across, 0, columns).astype(jnp.bfloat16)
        send(part_send.at[at], part_recv.at[at], part_sems, (at,), to_y)
    arrived(mate_gated.at[1], mate_sems, (1,))
    for at in range(count):
        columns = slice(at * cols_out, (at + 1) * cols_out)
        acc[:, columns] = project(me, 1, columns)
    pump(2)
    for name in ("residual", "outg", "ing"):
        loads[name].wait()
    for at in range(count):
        columns = slice(at * cols_out, (at + 1) * cols_out)
        arrived(part_recv.at[at], part_sems, (at,))
        acc[:, columns] = acc[:, columns] + part_recv[at].astype(jnp.float32)
        if at == 1:
            pump(1)

    member = lambda parity, owner: parity * count + owner
    own = member(par, me)
    cut = block // 2
    for at in range(2):
        rows = slice(at * cut, (at + 1) * cut)
        mixed = acc[rows, :]
        scale = lax.rsqrt(jnp.mean(mixed * mixed, axis=-1, keepdims=True) + EPSILON)
        total = residual[rows, :].astype(jnp.float32) + mixed * scale * out_gain[...]
        total = total.astype(jnp.bfloat16)
        first_own[rows, :] = total
        long = total.astype(jnp.float32)
        scale = lax.rsqrt(jnp.mean(long * long, axis=-1, keepdims=True) + EPSILON)
        normed[own, rows, :] = (long * scale * in_gain[...]).astype(jnp.bfloat16)
        for slot, peer in ((0, to_mate), (1, to_y), (2, to_z)):
            spot = normed.at[own, rows, :]
            send(spot, spot, ag_sems, (slot, at), peer)
    z_weights(jnp.logical_not(inner_row), (2, 2), (2, 1), (2, 3))
    columns = pl.ds(pl.multiple_of(me * cols_out, cols_out), cols_out)
    first_cols[me] = first_own[:, columns]

    facing = 1 - par
    came = {
        0: member(par, mate), 1: member(par, across), 2: member(facing, me),
        3: member(par, corner), 4: member(facing, mate), 5: member(facing, across),
        6: member(facing, corner),
    }

    def take(slot, at, *onward):
        spot = normed.at[came[slot], at * cut : (at + 1) * cut, :]
        arrived(spot, ag_sems, (slot, at))
        for further, peer in onward:
            send(spot, spot, ag_sems, (further, at), peer)

    pump(2)
    take(1, 0, (3, to_mate))
    take(2, 0, (4, to_mate), (5, to_y))
    z_weights(inner_row, (2, 2))
    take(1, 1, (3, to_mate))
    pump(1)
    take(2, 1, (4, to_mate), (5, to_y))
    for slot, owner in ((0, mate), (1, across), (2, corner)):
        columns = pl.ds(pl.multiple_of(owner * cols_out, cols_out), cols_out)
        send(first_own.at[:, columns], first_cols.at[me], first_sems, (slot,), {"tp": owner})
    pump(1)
    for kind in range(3):
        loads[kind].wait()
    gathered(0)
    gathered(1)

    def mix(parity, at):
        base = pl.multiple_of(parity * count + 2 * at, 2)
        left_rows = normed[pl.ds(base, 2)].reshape(2 * block, width)
        gate = jnp.dot(left_rows, gate_w[...], preferred_element_type=jnp.float32)
        up = jnp.dot(left_rows, up_w[...], preferred_element_type=jnp.float32)
        gate = (gate / (1.0 + jnp.exp(-gate)) * up).astype(jnp.bfloat16)
        active[pl.ds(base, 2)] = gate.reshape(2, block, half)

    take(0, 0)
    take(0, 1)
    mix(par, chip)
    take(5, 0, (6, to_mate))
    take(3, 0)
    take(3, 1)
    mix(par, 1 - chip)
    take(5, 1, (6, to_mate))
    take(4, 0)
    take(4, 1)
    mix(facing, chip)
    pump(1)
    take(6, 0)
    take(6, 1)
    mix(facing, 1 - chip)
    pump(1)

    side = cols_out // 2
    slim = side // 2
    targets = ((facing, 1 - chip), (par, 1 - chip), (facing, chip), (par, chip))

    def term(stage, parity, owner):
        base = pl.multiple_of(parity * count, count)
        left_rows = active[pl.ds(base, count)].reshape(rows_all, half)
        column = col if stage == 0 else 1 - col
        return jnp.dot(
            left_rows, down_w[2 * owner + column], preferred_element_type=jnp.float32
        )

    def for_mate(stage, at):
        parity, there = targets[at]
        to_core[stage, at] = term(stage, parity, 2 * there + 1 - core).astype(jnp.bfloat16)
        send(to_core.at[stage, at], from_core.at[stage, at], core_sems, (stage, at), to_mate)

    def summed(stage, at):
        parity, there = targets[at]
        part = term(stage, parity, 2 * there + core)
        arrived(from_core.at[stage, at], core_sems, (stage, at))
        part = part + from_core[stage, at].astype(jnp.float32)
        return part[:, :slim], part[:, slim:]

    def pass_on(stage, value_at, source, target, way, slot, peer):
        source[stage, slot] = value_at.astype(jnp.bfloat16)
        send(source.at[stage, slot], target.at[stage, slot], link_sems, (way, stage, slot), peer)

    def multiply(stage, between=lambda: None):
        for_mate(stage, 0)
        for_mate(stage, 1)
        low, top_part = summed(stage, 0)
        pass_on(stage, low, y_send, y_recv, 0, 0, to_y)
        pass_on(stage, top_part, z_send, z_recv, 1, 0, to_z)
        between()
        for_mate(stage, 2)
        low, top_part = summed(stage, 1)
        pass_on(stage, low, y_send, y_recv, 0, 1, to_y)
        held[stage, 0] = top_part
        for_mate(stage, 3)
        low, top_part = summed(stage, 2)
        held[stage, 1] = low
        pass_on(stage, top_part, z_send, z_recv, 1, 1, to_z)
        low, top_part = summed(stage, 3)
        kept[stage, :, :slim] = low
        kept[stage, :, slim:] = top_part

    def forward(stage):
        arrived(y_recv.at[stage, 0], link_sems, (0, stage, 0))
        pass_on(
            stage, held[stage, 1] + y_recv[stage, 0].astype(jnp.float32), z_send, z_recv, 1, 2,
            to_z,
        )
        arrived(z_recv.at[stage, 0], link_sems, (1, stage, 0))
        pass_on(
            stage, held[stage, 0] + z_recv[stage, 0].astype(jnp.float32), y_send, y_recv, 0, 2,
            to_y,
        )

    def deliver(stage):
        column = (col if stage == 0 else 1 - col) * side
        for at, one, two in ((0, y_recv, z_recv), (1, z_recv, y_recv)):
            way = at
            arrived(one.at[stage, 1], link_sems, (way, stage, 1))
            arrived(two.at[stage, 2], link_sems, (1 - way, stage, 2))
            columns = pl.ds(pl.multiple_of(column + at * slim, slim), slim)
            early = first_cols[:, :, columns].reshape(rows_all, slim).astype(jnp.float32)
            whole = kept[stage, :, at * slim : (at + 1) * slim]
            whole = whole + one[stage, 1].astype(jnp.float32) + two[stage, 2].astype(jnp.float32)
            out_ref[:, columns] = (early + 0.5 * whole).astype(jnp.bfloat16)

    multiply(0)
    gathered(2)
    multiply(1, lambda: forward(0))
    forward(1)
    for slot, owner in ((0, mate), (1, across), (2, corner)):
        arrived(first_cols.at[owner], first_sems, (slot,))
    deliver(0)
    deliver(1)
    for kind in range(3):
        for i in (1, 2, 3):
            z_copy(kind, i).wait_send()
    for copy in sent:
        copy.wait_send()
    for step in range(1, depth):

        @pl.when(row + step < depth)
        def _():
            for copy in plane_copies(step):
                copy.wait_send()


def paired(logs, cell_inputs, rows_inputs, weights):
    ranks, count = lax.axis_size("sp"), lax.axis_size("tp")
    heads = logs[0].shape[0]
    residual, out_gain, in_gain = rows_inputs
    projection, gate_weight, up_weight, down_weight = weights
    rows, width = residual.shape
    inner = projection.shape[0]
    half = gate_weight.shape[1] // 2
    cols = width // count
    block, side, depth = rows // count, cols // 2, ranks // 2
    dma = pltpu.SemaphoreType.DMA

    def low(*shape):
        return pltpu.VMEM(shape, jnp.bfloat16)

    def full(*shape):
        return pltpu.VMEM(shape, jnp.float32)

    like = lambda array: pltpu.VMEM(array.shape, array.dtype)
    members = 2 * count
    operands = (*logs, *cell_inputs, residual, out_gain, in_gain, *weights)
    return pl.pallas_call(
        functools.partial(pair_kernel, ranks, count, heads),
        out_shape=jax.ShapeDtypeStruct((rows, cols), jnp.bfloat16),
        in_specs=[ANY] * len(operands),
        out_specs=VMEM,
        scratch_shapes=[
            *(like(array) for array in (*logs, *cell_inputs)),
            low(block, width), full(1, width), full(1, width),
            low(inner, width), low(inner, width),
            low(width, half), low(width, half), low(ranks, half, down_weight.shape[1]),
            full(heads, rows), full(rows, 128),
            full(heads, DQK, DV), low(heads, DQK, DV), full(heads, 8, DQK),
            low(DQK, DV), full(8, DQK),
            full(DQK, DV), full(8, DQK),
            low(DQK, DV), full(8, DQK),
            low(depth - 1, DQK, DV), full(depth - 1, 8, DQK),
            full(DQK, DV), full(8, DQK),
            low(DQK, DV), full(8, DQK),
            low(heads, DQK, DV), full(heads, 8, DQK),
            full(rows, inner), low(rows, inner), low(2, block, inner),
            low(count, block, cols), low(count, block, cols), full(block, width),
            low(block, width), low(count, block, cols),
            low(members, block, width), low(members, block, half),
            low(2, 4, rows, side), low(2, 4, rows, side),
            *(low(2, 3, rows, side // 2) for _ in range(4)),
            full(2, 2, rows, side // 2), full(2, rows, side),
            dma((15,)), dma((2, 3, 2, depth)), dma((2, 4)), dma((2, 2, depth - 1)), dma((2, 3)),
            dma((2, count)), dma((2, 7, 2)), dma((2, 3)), dma((2, 2, 4)), dma((2, 2, 2, 3)),
        ],
        compiler_params=pltpu.CompilerParams(
            collective_id=0, has_side_effects=True, vmem_limit_bytes=VMEM_BYTES
        ),
        name="layer",
    )(*operands)


def body(
    residual,
    query_matrix,
    key_matrix,
    value_matrix,
    output_gate_logit,
    input_gate_log,
    forget_gate_logit,
    extra_head_decay,
    head_norm_gain,
    projection,
    cell_output_gain,
    mixer_input_gain,
    mixer_gate_weight,
    mixer_up_weight,
    mixer_down_weight,
):
    heads_here = input_gate_log.shape[1]
    if (lax.axis_size("sp"), lax.axis_size("tp"), heads_here) == (8, 4, 2):
        return paired(
            (forget_gate_logit.T, extra_head_decay.T, input_gate_log.T),
            (query_matrix, key_matrix, value_matrix, output_gate_logit, head_norm_gain[None]),
            (residual, cell_output_gain[None], mixer_input_gain[None]),
            (projection, mixer_gate_weight, mixer_up_weight, mixer_down_weight),
        )
    key_low = heads_first(key_matrix, heads_here, DQK)
    value_low = heads_first(value_matrix, heads_here, DV)
    keyed = key_low.astype(jnp.float32)
    valued = value_low.astype(jnp.float32)
    in_logs = input_gate_log.T
    running_log_total = jnp.cumsum(
        (jax.nn.log_sigmoid(forget_gate_logit) + extra_head_decay).T, axis=-1
    )
    zero_memory = jnp.zeros((heads_here, DV, DQK), jnp.float32)
    zero_normalizer = jnp.zeros((heads_here, DQK), jnp.float32)
    lowest = jnp.full((heads_here,), LOWEST_LOG, jnp.float32)
    local_memory, local_normalizer, local_max = fold_state(
        keyed, valued, in_logs, running_log_total, zero_memory, zero_normalizer, lowest
    )
    return layer(
        (running_log_total[:, -1], local_memory, local_normalizer, local_max),
        (running_log_total, in_logs),
        (query_matrix, key_matrix, value_matrix, output_gate_logit, head_norm_gain[None]),
        residual,
        (cell_output_gain[None], mixer_input_gain[None]),
        (projection, mixer_gate_weight, mixer_up_weight, mixer_down_weight),
    )


def solution(mesh):
    return jax.shard_map(
        body,
        mesh=mesh,
        in_specs=(
            P("sp", None),
            P("sp", "tp"),
            P("sp", "tp"),
            P("sp", "tp"),
            P("sp", "tp"),
            P("sp", "tp"),
            P("sp", "tp"),
            P("sp", "tp"),
            P("tp"),
            P("tp", None),
            P(),
            P(),
            P("sp", "tp"),
            P("sp", "tp"),
            P("tp", "sp"),
        ),
        out_specs=P("sp", "tp"),
        check_vma=False,
    )
```

```python
import functools

import jax
import jax.numpy as jnp
from jax import lax
from jax.experimental import pallas as pl
from jax.experimental.pallas import tpu as pltpu
from jax.sharding import PartitionSpec as P

DQK = 128
DV = 256
MESH = pl.DeviceIdType.MESH
VMEM = pl.BlockSpec(memory_space=pltpu.VMEM)
ANY = pl.BlockSpec(memory_space=pl.ANY)
VMEM_BYTES = 62 * 1024 * 1024

HIGHEST = lax.Precision.HIGHEST
EPSILON = 1e-06
LOWEST_LOG = -1e30


def heads_first(array, heads, width):
    return array.reshape(array.shape[0], heads, width).transpose(1, 0, 2)


def fold_state(keyed, valued, in_logs, running_log_total, memory, normalizer, stabilizer):
    last = running_log_total[:, -1]
    lifted = last[:, None] - running_log_total + in_logs
    new_max = jnp.maximum(last + stabilizer, jnp.max(lifted, axis=-1))
    weights = jnp.exp(lifted - new_max[:, None])
    retained = jnp.exp(last + stabilizer - new_max)
    memory = retained[:, None, None] * memory + jnp.einsum(
        "hsv,hsd->hvd", weights[:, :, None] * valued, keyed, precision=HIGHEST
    )
    normalizer = retained[:, None] * normalizer + jnp.einsum(
        "hs,hsd->hd", weights, keyed, precision=HIGHEST
    )
    return (memory, normalizer, new_max)


def copy_to(source, target, sems, slot, peer):
    return pltpu.make_async_remote_copy(
        source, target, sems.at[(0, *slot)], sems.at[(1, *slot)], device_id=peer, device_id_type=MESH
    )


def layer_kernel(
    ranks, count, heads, memory_ref, aux_ref, cum_row, in_row, cum_col, query_ref,
    key_ref, value_ref, ogate_ref, head_gain, residual_ref, out_gain, in_gain, projection_ref,
    gate_ref, up_ref, down_ref, out_ref, slots, aux_slots, memory, aux, gate_w, up_w, down_w,
    weight, gated, blocks, normed, first, active, to_core, from_core, to_chip, from_chip,
    state_sems, aux_sems, local_sems, proj_sems, gated_sems, sum_sems,
):
    sp, me = lax.axis_index("sp"), lax.axis_index("tp")
    core = lax.rem(me, 2)
    mate = me + 1 - 2 * core
    chips = count // 2
    rows_all, width = residual_ref.shape
    cols = out_ref.shape[1]
    inner = value_ref.shape[1]

    barrier = pltpu.get_barrier_semaphore()
    for axis, size, at in (("sp", ranks, sp), ("tp", count, me)):
        for step in range(1, size):
            pl.semaphore_signal(
                barrier, inc=1, device_id={axis: lax.rem(at + step, size)}, device_id_type=MESH
            )
    pl.semaphore_wait(barrier, ranks + count - 2)

    def state_copies(step):
        peer = {"sp": lax.rem(sp + step, ranks)}
        return (
            copy_to(memory_ref, slots.at[step - 1], state_sems, (step - 1,), peer),
            copy_to(aux_ref, aux_slots.at[step - 1], aux_sems, (step - 1,), peer),
        )

    for step in range(1, ranks):

        @pl.when(sp + step < ranks)
        def _():
            for copy in state_copies(step):
                copy.start()

    def spread(source, whole, sems):
        sent = [copy_to(source, whole.at[me], sems, (0,), {"tp": mate})]
        for step in range(1, chips):
            peer = {"tp": lax.rem(me + 2 * step, count)}
            sent.append(copy_to(source, whole.at[me], sems, (2 * step,), peer))
        for copy in sent:
            copy.start()
        return sent

    def relay(whole, sems):
        sent = []
        for step in range(1, chips):
            owner = lax.rem(me - 2 * step + count, count)
            block = whole.at[owner]
            copy_to(block, block, sems, (2 * step,), {"tp": mate}).wait_recv()
            sent.append(copy_to(block, block, sems, (2 * step - 1,), {"tp": mate}))
            sent[-1].start()
        return sent

    def collect(whole, sems):
        for step in range(chips):
            owner = lax.rem(mate - 2 * step + count, count)
            block = whole.at[owner]
            slot = 0 if step == 0 else 2 * step - 1
            copy_to(block, block, sems, (slot,), {"tp": mate}).wait_recv()

    for ref, whole, at in ((gate_ref, gate_w, 0), (up_ref, up_w, 1)):
        pltpu.make_async_copy(ref, whole, local_sems.at[at]).start()
    pltpu.make_async_copy(down_ref, down_w.at[0], local_sems.at[2]).start()
    own_weight = pltpu.make_async_copy(projection_ref, weight.at[me], local_sems.at[4])
    own_weight.start()
    sent = spread(projection_ref, weight, proj_sems)

    memory[...] = jnp.zeros_like(memory)
    aux[...] = jnp.zeros_like(aux)
    aux[heads : 2 * heads, :] = jnp.full((heads, DQK), LOWEST_LOG, jnp.float32)
    for step in range(ranks - 1, 0, -1):

        @pl.when(sp >= step)
        def _():
            for copy in state_copies(step):
                copy.wait_recv()
            late = aux_slots[step - 1]
            for head in range(heads):
                rows = pl.ds(head * DV, DV)
                early_max = aux[heads + head : heads + head + 1, :]
                late_max = late[heads + head : heads + head + 1, :]
                late_decay = late[2 * heads + head : 2 * heads + head + 1, :]
                joined = jnp.maximum(late_decay + early_max, late_max)
                before = jnp.exp(late_decay + early_max - joined)
                after = jnp.exp(late_max - joined)
                memory[rows, :] = before * memory[rows, :] + after * slots[
                    step - 1, rows, :
                ].astype(jnp.float32)
                aux[head : head + 1, :] = (
                    before * aux[head : head + 1, :] + after * late[head : head + 1, :]
                )
                aux[heads + head : heads + head + 1, :] = joined
                aux[2 * heads + head : 2 * heads + head + 1, :] = (
                    aux[2 * heads + head : 2 * heads + head + 1, :] + late_decay
                )

    tile = rows_all // 3
    for head in range(heads):
        prior_max = aux[heads + head : heads + head + 1, :]
        start_max = jnp.maximum(aux[2 * heads + head : 2 * heads + head + 1, :], prior_max)
        lift = jnp.exp(prior_max - start_max) * DQK ** (-0.5)
        memory[head * DV : (head + 1) * DV, :] = memory[head * DV : (head + 1) * DV, :] * lift
        aux[head : head + 1, :] = aux[head : head + 1, :] * lift
        aux[2 * heads + head : 2 * heads + head + 1, :] = start_max

    def read(at, unused):
        start = pl.multiple_of(at * tile, tile)
        rows = pl.ds(start, tile)
        causal = start + lax.broadcasted_iota(
            jnp.int32, (tile, rows_all), 0
        ) >= lax.broadcasted_iota(jnp.int32, (tile, rows_all), 1)
        for head in range(heads):
            keys = slice(head * DQK, (head + 1) * DQK)
            values = slice(head * DV, (head + 1) * DV)
            query = query_ref[rows, keys]
            total = cum_col[rows, head : head + 1]
            spread_log = total - cum_row[head : head + 1, :] + in_row[head : head + 1, :]
            spread_log = jnp.where(causal, spread_log, -jnp.inf)
            carried = total + aux[2 * heads + head : 2 * heads + head + 1, :1]
            running = jnp.maximum(carried, jnp.max(spread_log, axis=-1, keepdims=True))
            scores = lax.dot_general(
                query, key_ref[:, keys], (((1,), (1,)), ((), ())),
                preferred_element_type=jnp.float32,
            ) * DQK ** (-0.5)
            weights = jnp.exp(spread_log - running) * scores
            scaled = jnp.exp(carried - running)
            wide = query.astype(jnp.float32)
            numerator = jnp.dot(
                weights.astype(jnp.bfloat16), value_ref[:, values],
                preferred_element_type=jnp.float32,
            ) + scaled * lax.dot_general(
                wide, memory[values, :], (((1,), (1,)), ((), ())), precision=HIGHEST,
                preferred_element_type=jnp.float32,
            )
            denominator = jnp.sum(weights, axis=-1, keepdims=True) + scaled * jnp.sum(
                wide * aux[head : head + 1, :], axis=-1, keepdims=True
            )
            cell = numerator / jnp.maximum(jnp.abs(denominator), jnp.exp(-running))
            centered = cell - jnp.mean(cell, axis=-1, keepdims=True)
            cell = centered * lax.rsqrt(
                jnp.mean(centered * centered, axis=-1, keepdims=True) + EPSILON
            )
            cell = cell * head_gain[:, values]
            gate = ogate_ref[rows, values].astype(jnp.float32)
            gated[rows, values] = (cell * jax.nn.sigmoid(gate)).astype(jnp.bfloat16)
        return unused

    lax.fori_loop(0, 3, read, 0)
    sent += spread(gated, blocks, gated_sems)
    blocks[me] = gated[...]
    sent += relay(weight, proj_sems)
    sent += relay(blocks, gated_sems)
    collect(weight, proj_sems)
    own_weight.wait()
    collect(blocks, gated_sems)

    def turn(at, unused):
        rows = pl.ds(pl.multiple_of(at * tile, tile), tile)
        mixed = jnp.zeros((tile, width), jnp.float32)
        for block in range(count):
            mixed = mixed + jnp.dot(
                blocks[block, rows, :], weight[block], preferred_element_type=jnp.float32
            )
        scale = lax.rsqrt(jnp.mean(mixed * mixed, axis=-1, keepdims=True) + EPSILON)
        total = residual_ref[rows, :].astype(jnp.float32) + mixed * scale * out_gain[...]
        total = total.astype(jnp.bfloat16)
        first[rows, :] = total
        wide = total.astype(jnp.float32)
        scale = lax.rsqrt(jnp.mean(wide * wide, axis=-1, keepdims=True) + EPSILON)
        normed[rows, :] = (wide * scale * in_gain[...]).astype(jnp.bfloat16)
        return unused

    lax.fori_loop(0, 3, turn, 0)

    for ref, whole, at in ((gate_ref, gate_w, 0), (up_ref, up_w, 1)):
        pltpu.make_async_copy(ref, whole, local_sems.at[at]).wait()

    def mix(at, unused):
        rows = pl.ds(pl.multiple_of(at * tile, tile), tile)
        left = normed[rows, :]
        gate = jnp.dot(left, gate_w[...], preferred_element_type=jnp.float32)
        up = jnp.dot(left, up_w[...], preferred_element_type=jnp.float32)
        active[rows, :] = (gate / (1.0 + jnp.exp(-gate)) * up).astype(jnp.bfloat16)
        return unused

    lax.fori_loop(0, 3, mix, 0)
    pltpu.make_async_copy(down_ref, down_w.at[0], local_sems.at[2]).wait()

    def term(target):
        start = pl.multiple_of(target * cols, cols)
        return jnp.dot(
            active[...], down_w[0, :, pl.ds(start, cols)], preferred_element_type=jnp.float32
        )

    def send(source, target, kind, at, peer):
        return copy_to(source.at[at], target.at[at], sum_sems.at[kind], (at,), {"tp": peer})

    copies = []
    for step in range(1, chips):
        away = lax.rem(me + 2 * step, count)
        to_core[step] = term(away + 1 - 2 * core).astype(jnp.bfloat16)
        hop = send(to_core, from_core, 0, step, mate)
        hop.start()
        mine = term(away)
        hop.wait_recv()
        to_chip[step] = (mine + from_core[step].astype(jnp.float32)).astype(jnp.bfloat16)
        far = send(to_chip, from_chip, 1, step, away)
        far.start()
        copies += [hop, far]
    to_core[0] = term(mate).astype(jnp.bfloat16)
    hop = send(to_core, from_core, 0, 0, mate)
    hop.start()
    result = term(me)
    hop.wait_recv()
    result = result + from_core[0].astype(jnp.float32)
    for far in copies[1::2]:
        far.wait_recv()
    for step in range(1, chips):
        result = result + from_chip[step].astype(jnp.float32)
    own_first = first[:, pl.ds(pl.multiple_of(me * cols, cols), cols)]
    out_ref[...] = (own_first.astype(jnp.float32) + 0.5 * result).astype(jnp.bfloat16)
    for copy in copies + [hop] + sent:
        copy.wait_send()
    for step in range(1, ranks):

        @pl.when(sp + step < ranks)
        def _():
            for copy in state_copies(step):
                copy.wait_send()


def layer(states, logs, cell_inputs, residual, gains, weights):
    decay, memory, normalizer, maximum = states
    running_log_total, in_logs = logs
    ranks, count = lax.axis_size("sp"), lax.axis_size("tp")
    heads = decay.shape[0]
    rows, width = residual.shape
    projection, gate_weight, up_weight, down_weight = weights
    hidden = gate_weight.shape[1]
    inner = projection.shape[0]
    gate_weight = lax.all_gather(gate_weight, "sp", axis=0, tiled=True)
    up_weight = lax.all_gather(up_weight, "sp", axis=0, tiled=True)
    down_weight = lax.all_gather(down_weight, "sp", axis=1, tiled=True)
    down_shape = (1, hidden, width)
    fill = lambda row: jnp.broadcast_to(row[:, None], (heads, DQK))
    aux = jnp.concatenate([normalizer, fill(maximum), fill(decay)])
    height = -(-3 * heads // 8) * 8
    aux = jnp.pad(aux, ((0, height - 3 * heads), (0, 0)))
    low = memory.reshape(heads * DV, DQK).astype(jnp.bfloat16)
    chips, cols = count // 2, width // count
    buffer = pltpu.VMEM((chips, rows, cols), jnp.bfloat16)
    dma = pltpu.SemaphoreType.DMA
    return pl.pallas_call(
        functools.partial(layer_kernel, ranks, count, heads),
        out_shape=jax.ShapeDtypeStruct((rows, cols), jnp.bfloat16),
        in_specs=[VMEM] * 13 + [ANY] * 4,
        out_specs=VMEM,
        scratch_shapes=[
            pltpu.VMEM((ranks - 1, heads * DV, DQK), jnp.bfloat16),
            pltpu.VMEM((ranks - 1, height, DQK), jnp.float32),
            pltpu.VMEM((heads * DV, DQK), jnp.float32),
            pltpu.VMEM((height, DQK), jnp.float32),
            pltpu.VMEM((width, hidden), jnp.bfloat16),
            pltpu.VMEM((width, hidden), jnp.bfloat16),
            pltpu.VMEM(down_shape, jnp.bfloat16),
            pltpu.VMEM((count, inner, width), jnp.bfloat16),
            pltpu.VMEM((rows, inner), jnp.bfloat16),
            pltpu.VMEM((count, rows, inner), jnp.bfloat16),
            pltpu.VMEM((rows, width), jnp.bfloat16),
            pltpu.VMEM((rows, width), jnp.bfloat16),
            pltpu.VMEM((rows, hidden), jnp.bfloat16),
            buffer, buffer, buffer, buffer,
            dma((2, ranks - 1)),
            dma((2, ranks - 1)),
            dma((5,)),
            dma((2, count)),
            dma((2, count)),
            dma((2, 2, chips)),
        ],
        compiler_params=pltpu.CompilerParams(
            collective_id=0, has_side_effects=True, vmem_limit_bytes=VMEM_BYTES
        ),
        name="layer",
    )(
        low, aux, running_log_total, in_logs, running_log_total.T, *cell_inputs, residual,
        *gains, projection, gate_weight, up_weight, down_weight,
    )


def pair_kernel(
    ranks, count, heads, forget_hbm, extra_hbm, in_hbm, query_hbm, key_hbm, value_hbm, ogate_hbm,
    head_gain_hbm, residual_hbm, out_gain_hbm, in_gain_hbm, projection_hbm, gate_hbm, up_hbm,
    down_hbm, out_ref, forget, extra, in_row, query, key, value, ogate, head_gain, residual,
    out_gain, in_gain, proj_own, proj_mate, gate_w, up_w, down_w, cum_row, cols, own_mem, mem_send,
    aux, x_mem, x_aux, e_mem, e_aux, t_mem, t_aux, z_mem, z_aux, p_mem, p_aux, q_mem, q_aux,
    final_mem, final_aux, local, gated, mate_gated, part_send, part_recv, acc, first_own,
    first_cols, normed, active, to_core, from_core, y_send, y_recv, z_send, z_recv, ours, held, kept, result,
    local_sems, w_sems, state_sems, line_sems, mate_sems, part_sems, ag_sems, first_sems,
    core_sems, link_sems,
):
    sp, me = lax.axis_index("sp"), lax.axis_index("tp")
    row, col = sp // 2, lax.rem(sp, 2)
    depth = ranks // 2
    par = lax.rem(row, 2)
    core = lax.rem(me, 2)
    chip = me // 2
    mate = me + 1 - 2 * core
    across = lax.rem(me + 2, count)
    corner = lax.rem(mate + 2, count)
    rows_all, width = out_ref.shape[0], out_gain.shape[1]
    cols_out = out_ref.shape[1]
    block = rows_all // count
    half = gate_w.shape[1]
    quarter = half // 2
    high = gate_hbm.shape[0]
    others = {1: row + 1 - 2 * par, 2: lax.rem(row + 2, depth), 3: depth - 1 - row}
    inner_row = jnp.logical_or(row == 1, row == 2)
    to_x = {"sp": row * 2 + 1 - col}
    to_z = {"sp": others[1] * 2 + col}
    to_mate, to_y = {"tp": mate}, {"tp": across}
    sent = []

    barrier = pltpu.get_barrier_semaphore()
    greeted = [{"sp": others[i] * 2 + col} for i in (1, 2, 3)]
    greeted += [to_x, to_mate, to_y, {"tp": corner}]
    for peer in greeted:
        pl.semaphore_signal(barrier, inc=1, device_id=peer, device_id_type=MESH)

    loads = {}

    def load(name, source, target):
        loads[name] = pltpu.make_async_copy(source, target, local_sems.at[len(loads)])
        loads[name].start()

    load("forget", forget_hbm, forget)
    load("extra", extra_hbm, extra)
    load("in", in_hbm, in_row)
    load("key", key_hbm, key)
    load("value", value_hbm, value)
    load("query", query_hbm, query)
    load("ogate", ogate_hbm, ogate)
    load("head", head_gain_hbm, head_gain)
    load("proj", projection_hbm, proj_own)
    own_rows = pl.ds(pl.multiple_of(me * block, block), block)
    load("residual", residual_hbm.at[own_rows, :], residual)
    load("outg", out_gain_hbm, out_gain)
    load("ing", in_gain_hbm, in_gain)

    def piece(kind, parity):
        if kind >= 2:
            start = parity * half + (kind - 2) * quarter
            return down_hbm.at[pl.ds(pl.multiple_of(start, quarter), quarter), :]
        at = pl.ds(pl.multiple_of(parity * half, half), half)
        return (gate_hbm, up_hbm)[kind].at[:, at]

    def place(kind, owner):
        if kind >= 2:
            return down_w.at[owner, (kind - 2) * quarter : (kind - 1) * quarter, :]
        at = pl.ds(pl.multiple_of(owner * high, high), high)
        return (gate_w, up_w)[kind].at[at, :]

    for kind in range(4):
        load(kind, piece(kind, par), place(kind, sp))

    pl.semaphore_wait(barrier, len(greeted))

    def send(source, target, sems, slot, peer):
        copy = copy_to(source, target, sems, slot, peer)
        copy.start()
        sent.append(copy)

    def arrived(target, sems, slot):
        copy_to(target, target, sems, slot, to_mate).wait_recv()

    def z_copy(kind, i):
        there = others[i]
        return copy_to(
            piece(kind, lax.rem(there, 2)), place(kind, sp), w_sems, (kind, 0, i),
            {"sp": there * 2 + col},
        )

    def z_weights(condition, *pieces):
        @pl.when(condition)
        def _():
            for kind, i in pieces:
                z_copy(kind, i).start()

    def x_weights(kind):
        send(piece(kind, par), place(kind, sp), w_sems, (kind, 1, 0), to_x)

    relays = [(0, 1), (1, 1), (0, 3), (0, 2), (1, 3), (1, 2), (2, "soon"), (3, "soon")]
    relays += [(2, "late"), (3, "late"), (2, 2), (3, 2)]
    steps = {"soon": jnp.where(inner_row, 3, 1), "late": jnp.where(inner_row, 1, 3)}
    others |= {
        "soon": jnp.where(inner_row, others[3], others[1]),
        "late": jnp.where(inner_row, others[1], others[3]),
    }

    def pump(number):
        for _ in range(number):
            kind, i = relays.pop(0)
            spot = place(kind, others[i] * 2 + col)
            step = steps.get(i, i)
            arrived(spot, w_sems, (kind, 0, step))
            send(spot, spot, w_sems, (kind, 1, step), to_x)

    def gathered(kind):
        for i in range(depth):
            there = row if i == 0 else others[i]
            arrived(place(kind, there * 2 + 1 - col), w_sems, (kind, 1, i))

    odd, lower = par == 1, row < depth // 2
    z_weights(row >= 0, (0, 1))
    z_weights(row == 1, (0, 3))
    z_weights(odd, (1, 1))
    z_weights(jnp.logical_not(lower), (0, 3), (0, 2), (1, 3), (1, 2))
    z_weights(row == 1, (2, 1), (3, 1))
    z_weights(row == 2, (2, 3), (3, 3))
    send(projection_hbm, proj_mate, mate_sems, (2,), to_mate)

    for name in ("forget", "extra", "in"):
        loads[name].wait()
    logit = forget[...]
    decay = jnp.minimum(logit, 0.0) - jnp.log1p(jnp.exp(-jnp.abs(logit))) + extra[...]
    lane = lax.broadcasted_iota(jnp.int32, decay.shape, 1)
    shift = 1
    while shift < rows_all:
        decay = decay + jnp.where(lane >= shift, pltpu.roll(decay, shift, 1), 0.0)
        shift *= 2
    cum_row[...] = decay
    last = decay[:, rows_all - 1 : rows_all]
    lifted = last - decay + in_row[...]
    top = jnp.max(lifted, axis=-1, keepdims=True)
    lifted = jnp.exp(lifted - top)
    eye = lax.broadcasted_iota(jnp.int32, (128, 128), 0) == lax.broadcasted_iota(
        jnp.int32, (128, 128), 1
    )

    def to_column(line, at):
        for start in range(0, rows_all, 128):
            spread = jnp.broadcast_to(line[:, start : start + 128], (128, 128))
            cols[start : start + 128, at : at + 1] = jnp.sum(
                jnp.where(eye, spread, 0.0), axis=-1, keepdims=True
            )

    for head in range(heads):
        to_column(decay[head : head + 1, :], head)
        to_column(lifted[head : head + 1, :], heads + head)
    loads["key"].wait()
    loads["value"].wait()
    for head in range(heads):
        keys = slice(head * DQK, (head + 1) * DQK)
        values = slice(head * DV, (head + 1) * DV)
        share = cols[:, heads + head : heads + head + 1]
        heavy = (share * value[:, values].astype(jnp.float32)).astype(jnp.bfloat16)
        state = lax.dot_general(
            key[:, keys], heavy, (((0,), (0,)), ((), ())), preferred_element_type=jnp.float32
        )
        own_mem[head] = state
        mem_send[head] = state.astype(jnp.bfloat16)
        aux[head] = jnp.zeros((8, DQK), jnp.float32)
        aux[head, 0:1, :] = jnp.sum(
            share * key[:, keys].astype(jnp.float32), axis=0, keepdims=True
        )
        aux[head, 1:2, :] = jnp.broadcast_to(top[head : head + 1, :], (1, DQK))
        aux[head, 2:3, :] = jnp.broadcast_to(last[head : head + 1, :], (1, DQK))
    send(mem_send.at[1 - col], x_mem, state_sems, (0,), to_x)
    send(aux.at[1 - col], x_aux, state_sems, (1,), to_x)
    x_weights(0)

    tile = rows_all // 3
    loads["query"].wait()

    def nearby(head, at):
        start, reach = at * tile, (at + 1) * tile
        keys = slice(head * DQK, (head + 1) * DQK)
        values = slice(head * DV, (head + 1) * DV)
        rows = slice(start, reach)
        causal = start + lax.broadcasted_iota(
            jnp.int32, (tile, reach), 0
        ) >= lax.broadcasted_iota(jnp.int32, (tile, reach), 1)
        total = cols[rows, head : head + 1]
        spread_log = total - cum_row[head : head + 1, :reach] + in_row[head : head + 1, :reach]
        spread_log = jnp.where(causal, spread_log, -jnp.inf)
        running = jnp.max(spread_log, axis=-1, keepdims=True)
        scores = lax.dot_general(
            query[rows, keys], key[:reach, keys], (((1,), (1,)), ((), ())),
            preferred_element_type=jnp.float32,
        ) * DQK ** (-0.5)
        weights = jnp.exp(spread_log - running) * scores
        local[rows, values] = jnp.dot(
            weights.astype(jnp.bfloat16), value[:reach, values],
            preferred_element_type=jnp.float32,
        )
        cols[rows, 2 * heads + head : 2 * heads + head + 1] = running
        cols[rows, 3 * heads + head : 3 * heads + head + 1] = jnp.sum(
            weights, axis=-1, keepdims=True
        )

    nearby(0, 0)
    nearby(1, 0)
    nearby(0, 1)

    def parts(ref):
        return ref[0:1, :], ref[1:2, :], ref[2:3, :]

    def join(early_mem, early, late_mem, late):
        joined = jnp.maximum(late[2] + early[1], late[1])
        before = jnp.exp(late[2] + early[1] - joined)
        after = jnp.exp(late[1] - joined)
        memory = before[:, :1] * early_mem + after[:, :1] * late_mem
        return memory, (before * early[0] + after * late[0], joined, early[2] + late[2])

    def keep(ref, values):
        ref[...] = jnp.zeros(ref.shape, jnp.float32)
        for at, entry in enumerate(values):
            ref[at : at + 1, :] = entry

    left = col == 0
    arrived(x_mem, state_sems, (0,))
    arrived(x_aux, state_sems, (1,))
    mine, theirs = own_mem[col], x_mem[...].astype(jnp.float32)
    mine_aux = tuple(aux[col, at : at + 1, :] for at in range(3))
    theirs_aux = parts(x_aux)
    pick = lambda one, two: jnp.where(left, one, two)
    early_mem, late_mem = pick(mine, theirs), pick(theirs, mine)
    early_aux = tuple(pick(one, two) for one, two in zip(mine_aux, theirs_aux))
    late_aux = tuple(pick(two, one) for one, two in zip(mine_aux, theirs_aux))
    e_mem[...] = early_mem
    keep(e_aux, early_aux)
    both, both_aux = join(early_mem, early_aux, late_mem, late_aux)
    t_mem[...] = both.astype(jnp.bfloat16)
    keep(t_aux, both_aux)

    def plane_copies(step):
        peer = {"sp": lax.rem(sp + 2 * step, ranks)}
        return (
            copy_to(t_mem, z_mem.at[step - 1], line_sems, (0, step - 1), peer),
            copy_to(t_aux, z_aux.at[step - 1], line_sems, (1, step - 1), peer),
        )

    for step in range(depth - 1, 0, -1):

        @pl.when(row + step < depth)
        def _():
            for copy in plane_copies(step):
                copy.start()

    z_weights(par == 0, (1, 1))
    z_weights(row == 0, (0, 3))
    z_weights(lower, (0, 2), (1, 3), (1, 2))
    z_weights(row == 2, (2, 1), (3, 1))
    z_weights(row == 1, (2, 3), (3, 3))
    nearby(1, 1)
    nearby(0, 2)
    nearby(1, 2)

    p_mem[...] = jnp.zeros(p_mem.shape, jnp.float32)
    zero = jnp.zeros((1, DQK), jnp.float32)
    keep(p_aux, (zero, jnp.full((1, DQK), LOWEST_LOG, jnp.float32), zero))
    for step in range(depth - 1, 0, -1):

        @pl.when(row >= step)
        def _():
            for copy in plane_copies(step):
                copy.wait_recv()
            memory, rest = join(
                p_mem[...], parts(p_aux), z_mem[step - 1].astype(jnp.float32),
                parts(z_aux.at[step - 1]),
            )
            p_mem[...] = memory
            keep(p_aux, rest)

    prior, prior_aux = p_mem[...], parts(p_aux)
    more, more_aux = join(prior, prior_aux, e_mem[...], parts(e_aux))
    q_mem[...] = pick(more, prior).astype(jnp.bfloat16)
    keep(q_aux, tuple(pick(one, two) for one, two in zip(more_aux, prior_aux)))
    send(q_mem, final_mem.at[col], state_sems, (2,), to_x)
    send(q_aux, final_aux.at[col], state_sems, (3,), to_x)
    x_weights(1)
    x_weights(2)
    x_weights(3)
    final_mem[col] = pick(prior, more).astype(jnp.bfloat16)
    keep(final_aux.at[col], tuple(pick(two, one) for one, two in zip(more_aux, prior_aux)))
    loads["ogate"].wait()
    loads["head"].wait()
    arrived(final_mem.at[1 - col], state_sems, (2,))
    arrived(final_aux.at[1 - col], state_sems, (3,))

    for head in range(heads):
        keys = slice(head * DQK, (head + 1) * DQK)
        values = slice(head * DV, (head + 1) * DV)
        prior_max = final_aux[head, 1:2, :]
        start_max = jnp.maximum(final_aux[head, 2:3, :], prior_max)
        lift = (jnp.exp(prior_max - start_max) * DQK ** (-0.5))[:, :1]
        start_max = start_max[:, :1]
        for at in range(3):
            rows = slice(at * tile, (at + 1) * tile)
            question = query[rows, keys]
            found = cols[rows, 2 * heads + head : 2 * heads + head + 1]
            carried = cols[rows, head : head + 1] + start_max
            running = jnp.maximum(carried, found)
            inside = jnp.exp(found - running)
            scaled = jnp.exp(carried - running) * lift
            numerator = inside * local[rows, values] + scaled * jnp.dot(
                question, final_mem[head], preferred_element_type=jnp.float32
            )
            denominator = inside * cols[
                rows, 3 * heads + head : 3 * heads + head + 1
            ] + scaled * jnp.sum(
                question.astype(jnp.float32) * final_aux[head, 0:1, :], axis=-1, keepdims=True
            )
            cell = numerator / jnp.maximum(jnp.abs(denominator), jnp.exp(-running))
            centered = cell - jnp.mean(cell, axis=-1, keepdims=True)
            cell = centered * lax.rsqrt(
                jnp.mean(centered * centered, axis=-1, keepdims=True) + EPSILON
            )
            gate = ogate[rows, values].astype(jnp.float32)
            gated[rows, values] = (
                cell * head_gain[:, values] * jax.nn.sigmoid(gate)
            ).astype(jnp.bfloat16)

    def rows_of(owner):
        return pl.ds(pl.multiple_of(owner * block, block), block)

    send(gated.at[rows_of(corner), :], mate_gated.at[0], mate_sems, (0,), to_mate)
    send(gated.at[rows_of(mate), :], mate_gated.at[1], mate_sems, (1,), to_mate)
    loads["proj"].wait()
    arrived(proj_mate, mate_sems, (2,))

    def project(owner, slot, columns):
        return jnp.dot(
            gated[rows_of(owner), :], proj_own[:, columns], preferred_element_type=jnp.float32
        ) + jnp.dot(
            mate_gated[slot], proj_mate[:, columns], preferred_element_type=jnp.float32
        )

    arrived(mate_gated.at[0], mate_sems, (0,))
    for at in range(count):
        columns = slice(at * cols_out, (at + 1) * cols_out)
        part_send[at] = project(across, 0, columns).astype(jnp.bfloat16)
        send(part_send.at[at], part_recv.at[at], part_sems, (at,), to_y)
    arrived(mate_gated.at[1], mate_sems, (1,))
    for at in range(count):
        columns = slice(at * cols_out, (at + 1) * cols_out)
        acc[:, columns] = project(me, 1, columns)
    pump(1)
    for name in ("residual", "outg", "ing"):
        loads[name].wait()
    for at in range(count):
        columns = slice(at * cols_out, (at + 1) * cols_out)
        arrived(part_recv.at[at], part_sems, (at,))
        acc[:, columns] = acc[:, columns] + part_recv[at].astype(jnp.float32)
        if at < 2:
            pump(1)

    member = lambda parity, owner: parity * count + owner
    own = member(par, me)
    cut = block // 2
    for at in range(2):
        rows = slice(at * cut, (at + 1) * cut)
        mixed = acc[rows, :]
        scale = lax.rsqrt(jnp.mean(mixed * mixed, axis=-1, keepdims=True) + EPSILON)
        total = residual[rows, :].astype(jnp.float32) + mixed * scale * out_gain[...]
        total = total.astype(jnp.bfloat16)
        first_own[rows, :] = total
        long = total.astype(jnp.float32)
        scale = lax.rsqrt(jnp.mean(long * long, axis=-1, keepdims=True) + EPSILON)
        normed[own, rows, :] = (long * scale * in_gain[...]).astype(jnp.bfloat16)
        for slot, peer in ((0, to_mate), (1, to_y), (2, to_z)):
            spot = normed.at[own, rows, :]
            send(spot, spot, ag_sems, (slot, at), peer)
    z_weights(jnp.logical_not(inner_row), (2, 2), (3, 2), (2, 1), (3, 1), (2, 3), (3, 3))
    columns = pl.ds(pl.multiple_of(me * cols_out, cols_out), cols_out)
    first_cols[me] = first_own[:, columns]

    facing = 1 - par
    came = {
        0: member(par, mate), 1: member(par, across), 2: member(facing, me),
        3: member(par, corner), 4: member(facing, mate), 5: member(facing, across),
        6: member(facing, corner),
    }

    def take(slot, at, *onward):
        spot = normed.at[came[slot], at * cut : (at + 1) * cut, :]
        arrived(spot, ag_sems, (slot, at))
        for further, peer in onward:
            send(spot, spot, ag_sems, (further, at), peer)

    pump(2)
    take(1, 0, (3, to_mate))
    take(2, 0, (4, to_mate), (5, to_y))
    z_weights(inner_row, (2, 2), (3, 2))
    take(1, 1, (3, to_mate))
    pump(1)
    take(2, 1, (4, to_mate), (5, to_y))
    for slot, owner in ((0, mate), (1, across), (2, corner)):
        columns = pl.ds(pl.multiple_of(owner * cols_out, cols_out), cols_out)
        send(first_own.at[:, columns], first_cols.at[me], first_sems, (slot,), {"tp": owner})
    for kind in range(4):
        loads[kind].wait()
    gathered(0)
    gathered(1)

    def mix(parity, at):
        base = pl.multiple_of(parity * count + 2 * at, 2)
        left_rows = normed[pl.ds(base, 2)].reshape(2 * block, width)
        gate = jnp.dot(left_rows, gate_w[...], preferred_element_type=jnp.float32)
        up = jnp.dot(left_rows, up_w[...], preferred_element_type=jnp.float32)
        gate = (gate / (1.0 + jnp.exp(-gate)) * up).astype(jnp.bfloat16)
        active[pl.ds(base, 2)] = gate.reshape(2, block, half)

    take(0, 0)
    take(0, 1)
    mix(par, chip)
    take(5, 0, (6, to_mate))
    take(3, 0)
    take(3, 1)
    mix(par, 1 - chip)
    pump(2)
    take(4, 0)
    take(4, 1)
    mix(facing, chip)
    take(5, 1, (6, to_mate))
    take(6, 0)
    take(6, 1)
    mix(facing, 1 - chip)
    pump(4)

    side = cols_out // 2
    slim = side // 2
    targets = ((facing, 1 - chip), (par, 1 - chip), (facing, chip), (par, chip))

    def term(stage, parity, owner):
        base = pl.multiple_of(parity * count, count)
        left_rows = active[pl.ds(base, count)].reshape(rows_all, half)
        column = col if stage == 0 else 1 - col
        return jnp.dot(
            left_rows, down_w[2 * owner + column], preferred_element_type=jnp.float32
        )

    def both(stage, at):
        parity, there = targets[at]
        to_core[stage, at] = term(stage, parity, 2 * there + 1 - core).astype(jnp.bfloat16)
        ours[at] = term(stage, parity, 2 * there + core)
        send(to_core.at[stage, at], from_core.at[stage, at], core_sems, (stage, at), to_mate)

    def summed(stage, at):
        arrived(from_core.at[stage, at], core_sems, (stage, at))
        part = ours[at] + from_core[stage, at].astype(jnp.float32)
        return part[:, :slim], part[:, slim:]

    def pass_on(stage, value_at, source, target, way, slot, peer):
        source[stage, slot] = value_at.astype(jnp.bfloat16)
        send(source.at[stage, slot], target.at[stage, slot], link_sems, (way, stage, slot), peer)

    def multiply(stage):
        both(stage, 0)
        both(stage, 1)
        low, top_part = summed(stage, 0)
        pass_on(stage, low, y_send, y_recv, 0, 0, to_y)
        pass_on(stage, top_part, z_send, z_recv, 1, 0, to_z)
        both(stage, 2)
        low, top_part = summed(stage, 1)
        pass_on(stage, low, y_send, y_recv, 0, 1, to_y)
        held[stage, 0] = top_part
        both(stage, 3)
        low, top_part = summed(stage, 2)
        held[stage, 1] = low
        pass_on(stage, top_part, z_send, z_recv, 1, 1, to_z)
        low, top_part = summed(stage, 3)
        kept[stage, :, :slim] = low
        kept[stage, :, slim:] = top_part

    def forward(stage):
        arrived(y_recv.at[stage, 0], link_sems, (0, stage, 0))
        pass_on(
            stage, held[stage, 1] + y_recv[stage, 0].astype(jnp.float32), z_send, z_recv, 1, 2,
            to_z,
        )
        arrived(z_recv.at[stage, 0], link_sems, (1, stage, 0))
        pass_on(
            stage, held[stage, 0] + z_recv[stage, 0].astype(jnp.float32), y_send, y_recv, 0, 2,
            to_y,
        )

    def deliver(stage):
        column = (col if stage == 0 else 1 - col) * side
        for at, one, two in ((0, y_recv, z_recv), (1, z_recv, y_recv)):
            way = at
            arrived(one.at[stage, 1], link_sems, (way, stage, 1))
            arrived(two.at[stage, 2], link_sems, (1 - way, stage, 2))
            columns = pl.ds(pl.multiple_of(column + at * slim, slim), slim)
            early = first_cols[:, :, columns].reshape(rows_all, slim).astype(jnp.float32)
            whole = kept[stage, :, at * slim : (at + 1) * slim]
            whole = whole + one[stage, 1].astype(jnp.float32) + two[stage, 2].astype(jnp.float32)
            result[:, columns] = (early + 0.5 * whole).astype(jnp.bfloat16)
            written = pltpu.make_async_copy(
                result.at[:, columns], out_ref.at[:, columns], local_sems.at[16 + 2 * stage + at]
            )
            written.start()
            writes.append(written)

    before = len(sent)
    multiply(0)
    forward(0)
    gathered(2)
    gathered(3)
    multiply(1)
    forward(1)
    for slot, owner in ((0, mate), (1, across), (2, corner)):
        arrived(first_cols.at[owner], first_sems, (slot,))
    writes = []
    for kind in range(4):
        for i in (1, 2, 3):
            z_copy(kind, i).wait_send()
    for step in range(1, depth):

        @pl.when(row + step < depth)
        def _():
            for copy in plane_copies(step):
                copy.wait_send()

    for copy in sent[:before]:
        copy.wait_send()
    deliver(0)
    deliver(1)
    for copy in sent[before:]:
        copy.wait_send()
    for copy in writes:
        copy.wait()


def paired(logs, cell_inputs, rows_inputs, weights):
    ranks, count = lax.axis_size("sp"), lax.axis_size("tp")
    heads = logs[0].shape[0]
    residual, out_gain, in_gain = rows_inputs
    projection, gate_weight, up_weight, down_weight = weights
    rows, width = residual.shape
    inner = projection.shape[0]
    half = gate_weight.shape[1] // 2
    cols = width // count
    block, side, depth = rows // count, cols // 2, ranks // 2
    dma = pltpu.SemaphoreType.DMA

    def low(*shape):
        return pltpu.VMEM(shape, jnp.bfloat16)

    def full(*shape):
        return pltpu.VMEM(shape, jnp.float32)

    like = lambda array: pltpu.VMEM(array.shape, array.dtype)
    members = 2 * count
    operands = (*logs, *cell_inputs, residual, out_gain, in_gain, *weights)
    return pl.pallas_call(
        functools.partial(pair_kernel, ranks, count, heads),
        out_shape=jax.ShapeDtypeStruct((rows, cols), jnp.bfloat16),
        in_specs=[ANY] * len(operands),
        out_specs=ANY,
        scratch_shapes=[
            *(like(array) for array in (*logs, *cell_inputs)),
            low(block, width), full(1, width), full(1, width),
            low(inner, width), low(inner, width),
            low(width, half), low(width, half), low(ranks, half, down_weight.shape[1]),
            full(heads, rows), full(rows, 128),
            full(heads, DQK, DV), low(heads, DQK, DV), full(heads, 8, DQK),
            low(DQK, DV), full(8, DQK),
            full(DQK, DV), full(8, DQK),
            low(DQK, DV), full(8, DQK),
            low(depth - 1, DQK, DV), full(depth - 1, 8, DQK),
            full(DQK, DV), full(8, DQK),
            low(DQK, DV), full(8, DQK),
            low(heads, DQK, DV), full(heads, 8, DQK),
            full(rows, inner), low(rows, inner), low(2, block, inner),
            low(count, block, cols), low(count, block, cols), full(block, width),
            low(block, width), low(count, block, cols),
            low(members, block, width), low(members, block, half),
            low(2, 4, rows, side), low(2, 4, rows, side),
            *(low(2, 3, rows, side // 2) for _ in range(4)),
            full(4, rows, side), full(2, 2, rows, side // 2), full(2, rows, side),
            low(rows, cols),
            dma((20,)), dma((2, 4, 2, depth)), dma((2, 4)), dma((2, 2, depth - 1)), dma((2, 3)),
            dma((2, count)), dma((2, 7, 2)), dma((2, 3)), dma((2, 2, 4)), dma((2, 2, 2, 3)),
        ],
        compiler_params=pltpu.CompilerParams(
            collective_id=0, has_side_effects=True, vmem_limit_bytes=VMEM_BYTES
        ),
        name="layer",
    )(*operands)


def body(
    residual,
    query_matrix,
    key_matrix,
    value_matrix,
    output_gate_logit,
    input_gate_log,
    forget_gate_logit,
    extra_head_decay,
    head_norm_gain,
    projection,
    cell_output_gain,
    mixer_input_gain,
    mixer_gate_weight,
    mixer_up_weight,
    mixer_down_weight,
):
    heads_here = input_gate_log.shape[1]
    if (lax.axis_size("sp"), lax.axis_size("tp"), heads_here) == (8, 4, 2):
        return paired(
            (forget_gate_logit.T, extra_head_decay.T, input_gate_log.T),
            (query_matrix, key_matrix, value_matrix, output_gate_logit, head_norm_gain[None]),
            (residual, cell_output_gain[None], mixer_input_gain[None]),
            (projection, mixer_gate_weight, mixer_up_weight, mixer_down_weight),
        )
    key_low = heads_first(key_matrix, heads_here, DQK)
    value_low = heads_first(value_matrix, heads_here, DV)
    keyed = key_low.astype(jnp.float32)
    valued = value_low.astype(jnp.float32)
    in_logs = input_gate_log.T
    running_log_total = jnp.cumsum(
        (jax.nn.log_sigmoid(forget_gate_logit) + extra_head_decay).T, axis=-1
    )
    zero_memory = jnp.zeros((heads_here, DV, DQK), jnp.float32)
    zero_normalizer = jnp.zeros((heads_here, DQK), jnp.float32)
    lowest = jnp.full((heads_here,), LOWEST_LOG, jnp.float32)
    local_memory, local_normalizer, local_max = fold_state(
        keyed, valued, in_logs, running_log_total, zero_memory, zero_normalizer, lowest
    )
    return layer(
        (running_log_total[:, -1], local_memory, local_normalizer, local_max),
        (running_log_total, in_logs),
        (query_matrix, key_matrix, value_matrix, output_gate_logit, head_norm_gain[None]),
        residual,
        (cell_output_gain[None], mixer_input_gain[None]),
        (projection, mixer_gate_weight, mixer_up_weight, mixer_down_weight),
    )


def solution(mesh):
    return jax.shard_map(
        body,
        mesh=mesh,
        in_specs=(
            P("sp", None),
            P("sp", "tp"),
            P("sp", "tp"),
            P("sp", "tp"),
            P("sp", "tp"),
            P("sp", "tp"),
            P("sp", "tp"),
            P("sp", "tp"),
            P("tp"),
            P("tp", None),
            P(),
            P(),
            P("sp", "tp"),
            P("sp", "tp"),
            P("tp", "sp"),
        ),
        out_specs=P("sp", "tp"),
        check_vma=False,
    )
```

```python
import functools

import jax
import jax.numpy as jnp
from jax import lax
from jax.experimental import pallas as pl
from jax.experimental.pallas import tpu as pltpu
from jax.sharding import PartitionSpec as P

DQK = 128
DV = 256
MESH = pl.DeviceIdType.MESH
VMEM = pl.BlockSpec(memory_space=pltpu.VMEM)
ANY = pl.BlockSpec(memory_space=pl.ANY)
VMEM_BYTES = 62 * 1024 * 1024

HIGHEST = lax.Precision.HIGHEST
EPSILON = 1e-06
LOWEST_LOG = -1e30


def heads_first(array, heads, width):
    return array.reshape(array.shape[0], heads, width).transpose(1, 0, 2)


def fold_state(keyed, valued, in_logs, running_log_total, memory, normalizer, stabilizer):
    last = running_log_total[:, -1]
    lifted = last[:, None] - running_log_total + in_logs
    new_max = jnp.maximum(last + stabilizer, jnp.max(lifted, axis=-1))
    weights = jnp.exp(lifted - new_max[:, None])
    retained = jnp.exp(last + stabilizer - new_max)
    memory = retained[:, None, None] * memory + jnp.einsum(
        "hsv,hsd->hvd", weights[:, :, None] * valued, keyed, precision=HIGHEST
    )
    normalizer = retained[:, None] * normalizer + jnp.einsum(
        "hs,hsd->hd", weights, keyed, precision=HIGHEST
    )
    return (memory, normalizer, new_max)


def copy_to(source, target, sems, slot, peer):
    return pltpu.make_async_remote_copy(
        source, target, sems.at[(0, *slot)], sems.at[(1, *slot)], device_id=peer, device_id_type=MESH
    )


def layer_kernel(
    ranks, count, heads, memory_ref, aux_ref, cum_row, in_row, cum_col, query_ref,
    key_ref, value_ref, ogate_ref, head_gain, residual_ref, out_gain, in_gain, projection_ref,
    gate_ref, up_ref, down_ref, out_ref, slots, aux_slots, memory, aux, gate_w, up_w, down_w,
    weight, gated, blocks, normed, first, active, to_core, from_core, to_chip, from_chip,
    state_sems, aux_sems, local_sems, proj_sems, gated_sems, sum_sems,
):
    sp, me = lax.axis_index("sp"), lax.axis_index("tp")
    core = lax.rem(me, 2)
    mate = me + 1 - 2 * core
    chips = count // 2
    rows_all, width = residual_ref.shape
    cols = out_ref.shape[1]
    inner = value_ref.shape[1]

    barrier = pltpu.get_barrier_semaphore()
    for axis, size, at in (("sp", ranks, sp), ("tp", count, me)):
        for step in range(1, size):
            pl.semaphore_signal(
                barrier, inc=1, device_id={axis: lax.rem(at + step, size)}, device_id_type=MESH
            )
    pl.semaphore_wait(barrier, ranks + count - 2)

    def state_copies(step):
        peer = {"sp": lax.rem(sp + step, ranks)}
        return (
            copy_to(memory_ref, slots.at[step - 1], state_sems, (step - 1,), peer),
            copy_to(aux_ref, aux_slots.at[step - 1], aux_sems, (step - 1,), peer),
        )

    for step in range(1, ranks):

        @pl.when(sp + step < ranks)
        def _():
            for copy in state_copies(step):
                copy.start()

    def spread(source, whole, sems):
        sent = [copy_to(source, whole.at[me], sems, (0,), {"tp": mate})]
        for step in range(1, chips):
            peer = {"tp": lax.rem(me + 2 * step, count)}
            sent.append(copy_to(source, whole.at[me], sems, (2 * step,), peer))
        for copy in sent:
            copy.start()
        return sent

    def relay(whole, sems):
        sent = []
        for step in range(1, chips):
            owner = lax.rem(me - 2 * step + count, count)
            block = whole.at[owner]
            copy_to(block, block, sems, (2 * step,), {"tp": mate}).wait_recv()
            sent.append(copy_to(block, block, sems, (2 * step - 1,), {"tp": mate}))
            sent[-1].start()
        return sent

    def collect(whole, sems):
        for step in range(chips):
            owner = lax.rem(mate - 2 * step + count, count)
            block = whole.at[owner]
            slot = 0 if step == 0 else 2 * step - 1
            copy_to(block, block, sems, (slot,), {"tp": mate}).wait_recv()

    for ref, whole, at in ((gate_ref, gate_w, 0), (up_ref, up_w, 1)):
        pltpu.make_async_copy(ref, whole, local_sems.at[at]).start()
    pltpu.make_async_copy(down_ref, down_w.at[0], local_sems.at[2]).start()
    own_weight = pltpu.make_async_copy(projection_ref, weight.at[me], local_sems.at[4])
    own_weight.start()
    sent = spread(projection_ref, weight, proj_sems)

    memory[...] = jnp.zeros_like(memory)
    aux[...] = jnp.zeros_like(aux)
    aux[heads : 2 * heads, :] = jnp.full((heads, DQK), LOWEST_LOG, jnp.float32)
    for step in range(ranks - 1, 0, -1):

        @pl.when(sp >= step)
        def _():
            for copy in state_copies(step):
                copy.wait_recv()
            late = aux_slots[step - 1]
            for head in range(heads):
                rows = pl.ds(head * DV, DV)
                early_max = aux[heads + head : heads + head + 1, :]
                late_max = late[heads + head : heads + head + 1, :]
                late_decay = late[2 * heads + head : 2 * heads + head + 1, :]
                joined = jnp.maximum(late_decay + early_max, late_max)
                before = jnp.exp(late_decay + early_max - joined)
                after = jnp.exp(late_max - joined)
                memory[rows, :] = before * memory[rows, :] + after * slots[
                    step - 1, rows, :
                ].astype(jnp.float32)
                aux[head : head + 1, :] = (
                    before * aux[head : head + 1, :] + after * late[head : head + 1, :]
                )
                aux[heads + head : heads + head + 1, :] = joined
                aux[2 * heads + head : 2 * heads + head + 1, :] = (
                    aux[2 * heads + head : 2 * heads + head + 1, :] + late_decay
                )

    tile = rows_all // 3
    for head in range(heads):
        prior_max = aux[heads + head : heads + head + 1, :]
        start_max = jnp.maximum(aux[2 * heads + head : 2 * heads + head + 1, :], prior_max)
        lift = jnp.exp(prior_max - start_max) * DQK ** (-0.5)
        memory[head * DV : (head + 1) * DV, :] = memory[head * DV : (head + 1) * DV, :] * lift
        aux[head : head + 1, :] = aux[head : head + 1, :] * lift
        aux[2 * heads + head : 2 * heads + head + 1, :] = start_max

    def read(at, unused):
        start = pl.multiple_of(at * tile, tile)
        rows = pl.ds(start, tile)
        causal = start + lax.broadcasted_iota(
            jnp.int32, (tile, rows_all), 0
        ) >= lax.broadcasted_iota(jnp.int32, (tile, rows_all), 1)
        for head in range(heads):
            keys = slice(head * DQK, (head + 1) * DQK)
            values = slice(head * DV, (head + 1) * DV)
            query = query_ref[rows, keys]
            total = cum_col[rows, head : head + 1]
            spread_log = total - cum_row[head : head + 1, :] + in_row[head : head + 1, :]
            spread_log = jnp.where(causal, spread_log, -jnp.inf)
            carried = total + aux[2 * heads + head : 2 * heads + head + 1, :1]
            running = jnp.maximum(carried, jnp.max(spread_log, axis=-1, keepdims=True))
            scores = lax.dot_general(
                query, key_ref[:, keys], (((1,), (1,)), ((), ())),
                preferred_element_type=jnp.float32,
            ) * DQK ** (-0.5)
            weights = jnp.exp(spread_log - running) * scores
            scaled = jnp.exp(carried - running)
            wide = query.astype(jnp.float32)
            numerator = jnp.dot(
                weights.astype(jnp.bfloat16), value_ref[:, values],
                preferred_element_type=jnp.float32,
            ) + scaled * lax.dot_general(
                wide, memory[values, :], (((1,), (1,)), ((), ())), precision=HIGHEST,
                preferred_element_type=jnp.float32,
            )
            denominator = jnp.sum(weights, axis=-1, keepdims=True) + scaled * jnp.sum(
                wide * aux[head : head + 1, :], axis=-1, keepdims=True
            )
            cell = numerator / jnp.maximum(jnp.abs(denominator), jnp.exp(-running))
            centered = cell - jnp.mean(cell, axis=-1, keepdims=True)
            cell = centered * lax.rsqrt(
                jnp.mean(centered * centered, axis=-1, keepdims=True) + EPSILON
            )
            cell = cell * head_gain[:, values]
            gate = ogate_ref[rows, values].astype(jnp.float32)
            gated[rows, values] = (cell * jax.nn.sigmoid(gate)).astype(jnp.bfloat16)
        return unused

    lax.fori_loop(0, 3, read, 0)
    sent += spread(gated, blocks, gated_sems)
    blocks[me] = gated[...]
    sent += relay(weight, proj_sems)
    sent += relay(blocks, gated_sems)
    collect(weight, proj_sems)
    own_weight.wait()
    collect(blocks, gated_sems)

    def turn(at, unused):
        rows = pl.ds(pl.multiple_of(at * tile, tile), tile)
        mixed = jnp.zeros((tile, width), jnp.float32)
        for block in range(count):
            mixed = mixed + jnp.dot(
                blocks[block, rows, :], weight[block], preferred_element_type=jnp.float32
            )
        scale = lax.rsqrt(jnp.mean(mixed * mixed, axis=-1, keepdims=True) + EPSILON)
        total = residual_ref[rows, :].astype(jnp.float32) + mixed * scale * out_gain[...]
        total = total.astype(jnp.bfloat16)
        first[rows, :] = total
        wide = total.astype(jnp.float32)
        scale = lax.rsqrt(jnp.mean(wide * wide, axis=-1, keepdims=True) + EPSILON)
        normed[rows, :] = (wide * scale * in_gain[...]).astype(jnp.bfloat16)
        return unused

    lax.fori_loop(0, 3, turn, 0)

    for ref, whole, at in ((gate_ref, gate_w, 0), (up_ref, up_w, 1)):
        pltpu.make_async_copy(ref, whole, local_sems.at[at]).wait()

    def mix(at, unused):
        rows = pl.ds(pl.multiple_of(at * tile, tile), tile)
        left = normed[rows, :]
        gate = jnp.dot(left, gate_w[...], preferred_element_type=jnp.float32)
        up = jnp.dot(left, up_w[...], preferred_element_type=jnp.float32)
        active[rows, :] = (gate / (1.0 + jnp.exp(-gate)) * up).astype(jnp.bfloat16)
        return unused

    lax.fori_loop(0, 3, mix, 0)
    pltpu.make_async_copy(down_ref, down_w.at[0], local_sems.at[2]).wait()

    def term(target):
        start = pl.multiple_of(target * cols, cols)
        return jnp.dot(
            active[...], down_w[0, :, pl.ds(start, cols)], preferred_element_type=jnp.float32
        )

    def send(source, target, kind, at, peer):
        return copy_to(source.at[at], target.at[at], sum_sems.at[kind], (at,), {"tp": peer})

    copies = []
    for step in range(1, chips):
        away = lax.rem(me + 2 * step, count)
        to_core[step] = term(away + 1 - 2 * core).astype(jnp.bfloat16)
        hop = send(to_core, from_core, 0, step, mate)
        hop.start()
        mine = term(away)
        hop.wait_recv()
        to_chip[step] = (mine + from_core[step].astype(jnp.float32)).astype(jnp.bfloat16)
        far = send(to_chip, from_chip, 1, step, away)
        far.start()
        copies += [hop, far]
    to_core[0] = term(mate).astype(jnp.bfloat16)
    hop = send(to_core, from_core, 0, 0, mate)
    hop.start()
    result = term(me)
    hop.wait_recv()
    result = result + from_core[0].astype(jnp.float32)
    for far in copies[1::2]:
        far.wait_recv()
    for step in range(1, chips):
        result = result + from_chip[step].astype(jnp.float32)
    own_first = first[:, pl.ds(pl.multiple_of(me * cols, cols), cols)]
    out_ref[...] = (own_first.astype(jnp.float32) + 0.5 * result).astype(jnp.bfloat16)
    for copy in copies + [hop] + sent:
        copy.wait_send()
    for step in range(1, ranks):

        @pl.when(sp + step < ranks)
        def _():
            for copy in state_copies(step):
                copy.wait_send()


def layer(states, logs, cell_inputs, residual, gains, weights):
    decay, memory, normalizer, maximum = states
    running_log_total, in_logs = logs
    ranks, count = lax.axis_size("sp"), lax.axis_size("tp")
    heads = decay.shape[0]
    rows, width = residual.shape
    projection, gate_weight, up_weight, down_weight = weights
    hidden = gate_weight.shape[1]
    inner = projection.shape[0]
    gate_weight = lax.all_gather(gate_weight, "sp", axis=0, tiled=True)
    up_weight = lax.all_gather(up_weight, "sp", axis=0, tiled=True)
    down_weight = lax.all_gather(down_weight, "sp", axis=1, tiled=True)
    down_shape = (1, hidden, width)
    fill = lambda row: jnp.broadcast_to(row[:, None], (heads, DQK))
    aux = jnp.concatenate([normalizer, fill(maximum), fill(decay)])
    height = -(-3 * heads // 8) * 8
    aux = jnp.pad(aux, ((0, height - 3 * heads), (0, 0)))
    low = memory.reshape(heads * DV, DQK).astype(jnp.bfloat16)
    chips, cols = count // 2, width // count
    buffer = pltpu.VMEM((chips, rows, cols), jnp.bfloat16)
    dma = pltpu.SemaphoreType.DMA
    return pl.pallas_call(
        functools.partial(layer_kernel, ranks, count, heads),
        out_shape=jax.ShapeDtypeStruct((rows, cols), jnp.bfloat16),
        in_specs=[VMEM] * 13 + [ANY] * 4,
        out_specs=VMEM,
        scratch_shapes=[
            pltpu.VMEM((ranks - 1, heads * DV, DQK), jnp.bfloat16),
            pltpu.VMEM((ranks - 1, height, DQK), jnp.float32),
            pltpu.VMEM((heads * DV, DQK), jnp.float32),
            pltpu.VMEM((height, DQK), jnp.float32),
            pltpu.VMEM((width, hidden), jnp.bfloat16),
            pltpu.VMEM((width, hidden), jnp.bfloat16),
            pltpu.VMEM(down_shape, jnp.bfloat16),
            pltpu.VMEM((count, inner, width), jnp.bfloat16),
            pltpu.VMEM((rows, inner), jnp.bfloat16),
            pltpu.VMEM((count, rows, inner), jnp.bfloat16),
            pltpu.VMEM((rows, width), jnp.bfloat16),
            pltpu.VMEM((rows, width), jnp.bfloat16),
            pltpu.VMEM((rows, hidden), jnp.bfloat16),
            buffer, buffer, buffer, buffer,
            dma((2, ranks - 1)),
            dma((2, ranks - 1)),
            dma((5,)),
            dma((2, count)),
            dma((2, count)),
            dma((2, 2, chips)),
        ],
        compiler_params=pltpu.CompilerParams(
            collective_id=0, has_side_effects=True, vmem_limit_bytes=VMEM_BYTES
        ),
        name="layer",
    )(
        low, aux, running_log_total, in_logs, running_log_total.T, *cell_inputs, residual,
        *gains, projection, gate_weight, up_weight, down_weight,
    )


def pair_kernel(
    ranks, count, heads, forget_hbm, extra_hbm, in_hbm, query_hbm, key_hbm, value_hbm, ogate_hbm,
    head_gain_hbm, residual_hbm, out_gain_hbm, in_gain_hbm, projection_hbm, gate_hbm, up_hbm,
    down_hbm, out_ref, forget, extra, in_row, query, key, value, ogate, head_gain, residual,
    out_gain, in_gain, proj_own, proj_mate, gate_w, up_w, down_w, cum_row, cols, own_mem, mem_send,
    aux, x_mem, x_aux, e_mem, e_aux, t_mem, t_aux, z_mem, z_aux, p_mem, p_aux, q_mem, q_aux,
    final_mem, final_aux, local, gated, mate_gated, part_send, part_recv, acc, first_own,
    first_cols, normed, active, to_core, from_core, y_send, y_recv, z_send, z_recv, ours, held, kept, result,
    local_sems, w_sems, state_sems, line_sems, mate_sems, part_sems, ag_sems, first_sems,
    core_sems, link_sems, out_sems,
):
    sp, me = lax.axis_index("sp"), lax.axis_index("tp")
    row, col = sp // 2, lax.rem(sp, 2)
    depth = ranks // 2
    par = lax.rem(row, 2)
    core = lax.rem(me, 2)
    chip = me // 2
    mate = me + 1 - 2 * core
    across = lax.rem(me + 2, count)
    corner = lax.rem(mate + 2, count)
    rows_all, width = out_ref.shape[0], out_gain.shape[1]
    cols_out = out_ref.shape[1]
    block = rows_all // count
    half = gate_w.shape[1]
    quarter = half // 2
    high = gate_hbm.shape[0]
    others = {1: row + 1 - 2 * par, 2: lax.rem(row + 2, depth), 3: depth - 1 - row}
    inner_row = jnp.logical_or(row == 1, row == 2)
    to_x = {"sp": row * 2 + 1 - col}
    to_z = {"sp": others[1] * 2 + col}
    to_mate, to_y = {"tp": mate}, {"tp": across}
    sent = []
    lanes = {
        id(w_sems): lambda slot: 3 * slot[1] + min(slot[0], 2), id(ag_sems): lambda slot: 6,
        id(part_sems): lambda slot: 7, id(core_sems): lambda slot: 8,
        id(link_sems): lambda slot: 9 + slot[0],
    }

    def outward(source, target, sems, slot, peer):
        if id(sems) not in lanes:
            return copy_to(source, target, sems, slot, peer)
        return pltpu.make_async_remote_copy(
            source, target, out_sems.at[lanes[id(sems)](slot)], sems.at[slot], device_id=peer,
            device_id_type=MESH,
        )

    def all_left(lane, whole):
        lane = out_sems.at[lane]
        pltpu.make_async_remote_copy(
            whole, whole, lane, lane, device_id=to_mate, device_id_type=MESH
        ).wait_send()

    barrier = pltpu.get_barrier_semaphore()
    greeted = [{"sp": others[i] * 2 + col} for i in (1, 2, 3)]
    greeted += [to_x, to_mate, to_y, {"tp": corner}]
    for peer in greeted:
        pl.semaphore_signal(barrier, inc=1, device_id=peer, device_id_type=MESH)

    loads = {}

    def load(name, source, target):
        loads[name] = pltpu.make_async_copy(source, target, local_sems.at[len(loads)])
        loads[name].start()

    load("forget", forget_hbm, forget)
    load("extra", extra_hbm, extra)
    load("in", in_hbm, in_row)
    load("key", key_hbm, key)
    load("value", value_hbm, value)
    load("query", query_hbm, query)
    load("ogate", ogate_hbm, ogate)
    load("head", head_gain_hbm, head_gain)
    load("proj", projection_hbm, proj_own)
    own_rows = pl.ds(pl.multiple_of(me * block, block), block)
    load("residual", residual_hbm.at[own_rows, :], residual)
    load("outg", out_gain_hbm, out_gain)
    load("ing", in_gain_hbm, in_gain)

    def piece(kind, parity):
        if kind >= 2:
            start = parity * half + (kind - 2) * quarter
            return down_hbm.at[pl.ds(pl.multiple_of(start, quarter), quarter), :]
        at = pl.ds(pl.multiple_of(parity * half, half), half)
        return (gate_hbm, up_hbm)[kind].at[:, at]

    def place(kind, owner):
        if kind >= 2:
            return down_w.at[owner, (kind - 2) * quarter : (kind - 1) * quarter, :]
        at = pl.ds(pl.multiple_of(owner * high, high), high)
        return (gate_w, up_w)[kind].at[at, :]

    for kind in range(4):
        load(kind, piece(kind, par), place(kind, sp))

    pl.semaphore_wait(barrier, len(greeted))

    def send(source, target, sems, slot, peer):
        copy = outward(source, target, sems, slot, peer)
        copy.start()
        if id(sems) not in lanes:
            sent.append(copy)

    def arrived(target, sems, slot):
        outward(target, target, sems, slot, to_mate).wait_recv()

    def z_copy(kind, i):
        there = others[i]
        return outward(
            piece(kind, lax.rem(there, 2)), place(kind, sp), w_sems, (kind, 0, i),
            {"sp": there * 2 + col},
        )

    def z_weights(condition, *pieces):
        @pl.when(condition)
        def _():
            for kind, i in pieces:
                z_copy(kind, i).start()

    def x_weights(kind):
        send(piece(kind, par), place(kind, sp), w_sems, (kind, 1, 0), to_x)

    relays = [(0, 1), (1, 1), (0, 3), (0, 2), (1, 3), (1, 2), (2, "soon"), (3, "soon")]
    relays += [(2, "late"), (3, "late"), (2, 2), (3, 2)]
    steps = {"soon": jnp.where(inner_row, 3, 1), "late": jnp.where(inner_row, 1, 3)}
    others |= {
        "soon": jnp.where(inner_row, others[3], others[1]),
        "late": jnp.where(inner_row, others[1], others[3]),
    }

    def pump(number):
        for _ in range(number):
            kind, i = relays.pop(0)
            spot = place(kind, others[i] * 2 + col)
            step = steps.get(i, i)
            arrived(spot, w_sems, (kind, 0, step))
            send(spot, spot, w_sems, (kind, 1, step), to_x)

    def gathered(kind):
        for i in range(depth):
            there = row if i == 0 else others[i]
            arrived(place(kind, there * 2 + 1 - col), w_sems, (kind, 1, i))

    odd, lower = par == 1, row < depth // 2
    z_weights(row >= 0, (0, 1))
    z_weights(row == 1, (0, 3))
    z_weights(odd, (1, 1))
    z_weights(jnp.logical_not(lower), (0, 3), (0, 2), (1, 3), (1, 2))
    z_weights(row == 1, (2, 1), (3, 1))
    z_weights(row == 2, (2, 3), (3, 3))
    send(projection_hbm, proj_mate, mate_sems, (2,), to_mate)

    for name in ("forget", "extra", "in"):
        loads[name].wait()
    logit = forget[...]
    decay = jnp.minimum(logit, 0.0) - jnp.log1p(jnp.exp(-jnp.abs(logit))) + extra[...]
    lane = lax.broadcasted_iota(jnp.int32, decay.shape, 1)
    shift = 1
    while shift < rows_all:
        decay = decay + jnp.where(lane >= shift, pltpu.roll(decay, shift, 1), 0.0)
        shift *= 2
    cum_row[...] = decay
    last = decay[:, rows_all - 1 : rows_all]
    lifted = last - decay + in_row[...]
    top = jnp.max(lifted, axis=-1, keepdims=True)
    lifted = jnp.exp(lifted - top)
    eye = lax.broadcasted_iota(jnp.int32, (128, 128), 0) == lax.broadcasted_iota(
        jnp.int32, (128, 128), 1
    )

    def to_column(line, at):
        for start in range(0, rows_all, 128):
            spread = jnp.broadcast_to(line[:, start : start + 128], (128, 128))
            cols[start : start + 128, at : at + 1] = jnp.sum(
                jnp.where(eye, spread, 0.0), axis=-1, keepdims=True
            )

    for head in range(heads):
        to_column(decay[head : head + 1, :], head)
        to_column(lifted[head : head + 1, :], heads + head)
    loads["key"].wait()
    loads["value"].wait()
    for head in range(heads):
        keys = slice(head * DQK, (head + 1) * DQK)
        values = slice(head * DV, (head + 1) * DV)
        share = cols[:, heads + head : heads + head + 1]
        heavy = (share * value[:, values].astype(jnp.float32)).astype(jnp.bfloat16)
        state = lax.dot_general(
            key[:, keys], heavy, (((0,), (0,)), ((), ())), preferred_element_type=jnp.float32
        )
        own_mem[head] = state
        mem_send[head] = state.astype(jnp.bfloat16)
        aux[head] = jnp.zeros((8, DQK), jnp.float32)
        aux[head, 0:1, :] = jnp.sum(
            share * key[:, keys].astype(jnp.float32), axis=0, keepdims=True
        )
        aux[head, 1:2, :] = jnp.broadcast_to(top[head : head + 1, :], (1, DQK))
        aux[head, 2:3, :] = jnp.broadcast_to(last[head : head + 1, :], (1, DQK))
    send(mem_send.at[1 - col], x_mem, state_sems, (0,), to_x)
    send(aux.at[1 - col], x_aux, state_sems, (1,), to_x)
    x_weights(0)

    tile = rows_all // 3
    loads["query"].wait()

    def nearby(head, at):
        start, reach = at * tile, (at + 1) * tile
        keys = slice(head * DQK, (head + 1) * DQK)
        values = slice(head * DV, (head + 1) * DV)
        rows = slice(start, reach)
        causal = start + lax.broadcasted_iota(
            jnp.int32, (tile, reach), 0
        ) >= lax.broadcasted_iota(jnp.int32, (tile, reach), 1)
        total = cols[rows, head : head + 1]
        spread_log = total - cum_row[head : head + 1, :reach] + in_row[head : head + 1, :reach]
        spread_log = jnp.where(causal, spread_log, -jnp.inf)
        running = jnp.max(spread_log, axis=-1, keepdims=True)
        scores = lax.dot_general(
            query[rows, keys], key[:reach, keys], (((1,), (1,)), ((), ())),
            preferred_element_type=jnp.float32,
        ) * DQK ** (-0.5)
        weights = jnp.exp(spread_log - running) * scores
        local[rows, values] = jnp.dot(
            weights.astype(jnp.bfloat16), value[:reach, values],
            preferred_element_type=jnp.float32,
        )
        cols[rows, 2 * heads + head : 2 * heads + head + 1] = running
        cols[rows, 3 * heads + head : 3 * heads + head + 1] = jnp.sum(
            weights, axis=-1, keepdims=True
        )

    nearby(0, 0)
    nearby(1, 0)
    nearby(0, 1)

    def parts(ref):
        return ref[0:1, :], ref[1:2, :], ref[2:3, :]

    def join(early_mem, early, late_mem, late):
        joined = jnp.maximum(late[2] + early[1], late[1])
        before = jnp.exp(late[2] + early[1] - joined)
        after = jnp.exp(late[1] - joined)
        memory = before[:, :1] * early_mem + after[:, :1] * late_mem
        return memory, (before * early[0] + after * late[0], joined, early[2] + late[2])

    def keep(ref, values):
        ref[...] = jnp.zeros(ref.shape, jnp.float32)
        for at, entry in enumerate(values):
            ref[at : at + 1, :] = entry

    left = col == 0
    arrived(x_mem, state_sems, (0,))
    arrived(x_aux, state_sems, (1,))
    mine, theirs = own_mem[col], x_mem[...].astype(jnp.float32)
    mine_aux = tuple(aux[col, at : at + 1, :] for at in range(3))
    theirs_aux = parts(x_aux)
    pick = lambda one, two: jnp.where(left, one, two)
    early_mem, late_mem = pick(mine, theirs), pick(theirs, mine)
    early_aux = tuple(pick(one, two) for one, two in zip(mine_aux, theirs_aux))
    late_aux = tuple(pick(two, one) for one, two in zip(mine_aux, theirs_aux))
    e_mem[...] = early_mem
    keep(e_aux, early_aux)
    both, both_aux = join(early_mem, early_aux, late_mem, late_aux)
    t_mem[...] = both.astype(jnp.bfloat16)
    keep(t_aux, both_aux)

    def plane_copies(step):
        peer = {"sp": lax.rem(sp + 2 * step, ranks)}
        return (
            copy_to(t_mem, z_mem.at[step - 1], line_sems, (0, step - 1), peer),
            copy_to(t_aux, z_aux.at[step - 1], line_sems, (1, step - 1), peer),
        )

    for step in range(depth - 1, 0, -1):

        @pl.when(row + step < depth)
        def _():
            for copy in plane_copies(step):
                copy.start()

    z_weights(par == 0, (1, 1))
    z_weights(row == 0, (0, 3))
    z_weights(lower, (0, 2), (1, 3), (1, 2))
    z_weights(row == 2, (2, 1), (3, 1))
    z_weights(row == 1, (2, 3), (3, 3))
    nearby(1, 1)
    nearby(0, 2)
    nearby(1, 2)

    p_mem[...] = jnp.zeros(p_mem.shape, jnp.float32)
    zero = jnp.zeros((1, DQK), jnp.float32)
    keep(p_aux, (zero, jnp.full((1, DQK), LOWEST_LOG, jnp.float32), zero))
    for step in range(depth - 1, 0, -1):

        @pl.when(row >= step)
        def _():
            for copy in plane_copies(step):
                copy.wait_recv()
            memory, rest = join(
                p_mem[...], parts(p_aux), z_mem[step - 1].astype(jnp.float32),
                parts(z_aux.at[step - 1]),
            )
            p_mem[...] = memory
            keep(p_aux, rest)

    prior, prior_aux = p_mem[...], parts(p_aux)
    more, more_aux = join(prior, prior_aux, e_mem[...], parts(e_aux))
    q_mem[...] = pick(more, prior).astype(jnp.bfloat16)
    keep(q_aux, tuple(pick(one, two) for one, two in zip(more_aux, prior_aux)))
    send(q_mem, final_mem.at[col], state_sems, (2,), to_x)
    send(q_aux, final_aux.at[col], state_sems, (3,), to_x)
    x_weights(1)
    x_weights(2)
    x_weights(3)
    final_mem[col] = pick(prior, more).astype(jnp.bfloat16)
    keep(final_aux.at[col], tuple(pick(two, one) for one, two in zip(more_aux, prior_aux)))
    loads["ogate"].wait()
    loads["head"].wait()
    arrived(final_mem.at[1 - col], state_sems, (2,))
    arrived(final_aux.at[1 - col], state_sems, (3,))

    for head in range(heads):
        keys = slice(head * DQK, (head + 1) * DQK)
        values = slice(head * DV, (head + 1) * DV)
        prior_max = final_aux[head, 1:2, :]
        start_max = jnp.maximum(final_aux[head, 2:3, :], prior_max)
        lift = (jnp.exp(prior_max - start_max) * DQK ** (-0.5))[:, :1]
        start_max = start_max[:, :1]
        for at in range(3):
            rows = slice(at * tile, (at + 1) * tile)
            question = query[rows, keys]
            found = cols[rows, 2 * heads + head : 2 * heads + head + 1]
            carried = cols[rows, head : head + 1] + start_max
            running = jnp.maximum(carried, found)
            inside = jnp.exp(found - running)
            scaled = jnp.exp(carried - running) * lift
            numerator = inside * local[rows, values] + scaled * jnp.dot(
                question, final_mem[head], preferred_element_type=jnp.float32
            )
            denominator = inside * cols[
                rows, 3 * heads + head : 3 * heads + head + 1
            ] + scaled * jnp.sum(
                question.astype(jnp.float32) * final_aux[head, 0:1, :], axis=-1, keepdims=True
            )
            cell = numerator / jnp.maximum(jnp.abs(denominator), jnp.exp(-running))
            centered = cell - jnp.mean(cell, axis=-1, keepdims=True)
            cell = centered * lax.rsqrt(
                jnp.mean(centered * centered, axis=-1, keepdims=True) + EPSILON
            )
            gate = ogate[rows, values].astype(jnp.float32)
            gated[rows, values] = (
                cell * head_gain[:, values] * jax.nn.sigmoid(gate)
            ).astype(jnp.bfloat16)

    def rows_of(owner):
        return pl.ds(pl.multiple_of(owner * block, block), block)

    send(gated.at[rows_of(corner), :], mate_gated.at[0], mate_sems, (0,), to_mate)
    send(gated.at[rows_of(mate), :], mate_gated.at[1], mate_sems, (1,), to_mate)
    loads["proj"].wait()
    arrived(proj_mate, mate_sems, (2,))

    def project(owner, slot, columns):
        return jnp.dot(
            gated[rows_of(owner), :], proj_own[:, columns], preferred_element_type=jnp.float32
        ) + jnp.dot(
            mate_gated[slot], proj_mate[:, columns], preferred_element_type=jnp.float32
        )

    arrived(mate_gated.at[0], mate_sems, (0,))
    for at in range(count):
        columns = slice(at * cols_out, (at + 1) * cols_out)
        part_send[at] = project(across, 0, columns).astype(jnp.bfloat16)
        send(part_send.at[at], part_recv.at[at], part_sems, (at,), to_y)
    arrived(mate_gated.at[1], mate_sems, (1,))
    for at in range(count):
        columns = slice(at * cols_out, (at + 1) * cols_out)
        acc[:, columns] = project(me, 1, columns)
    pump(1)
    for name in ("residual", "outg", "ing"):
        loads[name].wait()
    for at in range(count):
        columns = slice(at * cols_out, (at + 1) * cols_out)
        arrived(part_recv.at[at], part_sems, (at,))
        acc[:, columns] = acc[:, columns] + part_recv[at].astype(jnp.float32)
        if at < 2:
            pump(1)

    member = lambda parity, owner: parity * count + owner
    own = member(par, me)
    cut = block // 2
    for at in range(2):
        rows = slice(at * cut, (at + 1) * cut)
        mixed = acc[rows, :]
        scale = lax.rsqrt(jnp.mean(mixed * mixed, axis=-1, keepdims=True) + EPSILON)
        total = residual[rows, :].astype(jnp.float32) + mixed * scale * out_gain[...]
        total = total.astype(jnp.bfloat16)
        first_own[rows, :] = total
        long = total.astype(jnp.float32)
        scale = lax.rsqrt(jnp.mean(long * long, axis=-1, keepdims=True) + EPSILON)
        normed[own, rows, :] = (long * scale * in_gain[...]).astype(jnp.bfloat16)
        for slot, peer in ((0, to_mate), (1, to_y), (2, to_z)):
            spot = normed.at[own, rows, :]
            send(spot, spot, ag_sems, (slot, at), peer)
    z_weights(jnp.logical_not(inner_row), (2, 2), (3, 2), (2, 1), (3, 1), (2, 3), (3, 3))
    columns = pl.ds(pl.multiple_of(me * cols_out, cols_out), cols_out)
    first_cols[me] = first_own[:, columns]

    facing = 1 - par
    came = {
        0: member(par, mate), 1: member(par, across), 2: member(facing, me),
        3: member(par, corner), 4: member(facing, mate), 5: member(facing, across),
        6: member(facing, corner),
    }

    def take(slot, at, *onward):
        spot = normed.at[came[slot], at * cut : (at + 1) * cut, :]
        arrived(spot, ag_sems, (slot, at))
        for further, peer in onward:
            send(spot, spot, ag_sems, (further, at), peer)

    pump(2)
    take(1, 0, (3, to_mate))
    take(2, 0, (4, to_mate), (5, to_y))
    z_weights(inner_row, (2, 2), (3, 2))
    take(1, 1, (3, to_mate))
    pump(1)
    take(2, 1, (4, to_mate), (5, to_y))
    for slot, owner in ((0, mate), (1, across), (2, corner)):
        columns = pl.ds(pl.multiple_of(owner * cols_out, cols_out), cols_out)
        send(first_own.at[:, columns], first_cols.at[me], first_sems, (slot,), {"tp": owner})
    for kind in range(4):
        loads[kind].wait()
    gathered(0)
    gathered(1)

    def mix(parity, at):
        base = pl.multiple_of(parity * count + 2 * at, 2)
        left_rows = normed[pl.ds(base, 2)].reshape(2 * block, width)
        gate = jnp.dot(left_rows, gate_w[...], preferred_element_type=jnp.float32)
        up = jnp.dot(left_rows, up_w[...], preferred_element_type=jnp.float32)
        gate = (gate / (1.0 + jnp.exp(-gate)) * up).astype(jnp.bfloat16)
        active[pl.ds(base, 2)] = gate.reshape(2, block, half)

    take(0, 0)
    take(0, 1)
    mix(par, chip)
    take(5, 0, (6, to_mate))
    take(3, 0)
    take(3, 1)
    mix(par, 1 - chip)
    pump(2)
    take(4, 0)
    take(4, 1)
    mix(facing, chip)
    take(5, 1, (6, to_mate))
    take(6, 0)
    take(6, 1)
    mix(facing, 1 - chip)
    pump(4)

    side = cols_out // 2
    slim = side // 2
    targets = ((facing, 1 - chip), (par, 1 - chip), (facing, chip), (par, chip))

    def term(stage, parity, owner):
        base = pl.multiple_of(parity * count, count)
        left_rows = active[pl.ds(base, count)].reshape(rows_all, half)
        column = col if stage == 0 else 1 - col
        return jnp.dot(
            left_rows, down_w[2 * owner + column], preferred_element_type=jnp.float32
        )

    def both(stage, at):
        parity, there = targets[at]
        to_core[stage, at] = term(stage, parity, 2 * there + 1 - core).astype(jnp.bfloat16)
        ours[at] = term(stage, parity, 2 * there + core)
        send(to_core.at[stage, at], from_core.at[stage, at], core_sems, (stage, at), to_mate)

    def summed(stage, at):
        arrived(from_core.at[stage, at], core_sems, (stage, at))
        part = ours[at] + from_core[stage, at].astype(jnp.float32)
        return part[:, :slim], part[:, slim:]

    def pass_on(stage, value_at, source, target, way, slot, peer):
        source[stage, slot] = value_at.astype(jnp.bfloat16)
        send(source.at[stage, slot], target.at[stage, slot], link_sems, (way, stage, slot), peer)

    def multiply(stage):
        both(stage, 0)
        both(stage, 1)
        low, top_part = summed(stage, 0)
        pass_on(stage, low, y_send, y_recv, 0, 0, to_y)
        pass_on(stage, top_part, z_send, z_recv, 1, 0, to_z)
        both(stage, 2)
        low, top_part = summed(stage, 1)
        pass_on(stage, low, y_send, y_recv, 0, 1, to_y)
        held[stage, 0] = top_part
        both(stage, 3)
        low, top_part = summed(stage, 2)
        held[stage, 1] = low
        pass_on(stage, top_part, z_send, z_recv, 1, 1, to_z)
        low, top_part = summed(stage, 3)
        kept[stage, :, :slim] = low
        kept[stage, :, slim:] = top_part

    def forward(stage):
        arrived(y_recv.at[stage, 0], link_sems, (0, stage, 0))
        pass_on(
            stage, held[stage, 1] + y_recv[stage, 0].astype(jnp.float32), z_send, z_recv, 1, 2,
            to_z,
        )
        arrived(z_recv.at[stage, 0], link_sems, (1, stage, 0))
        pass_on(
            stage, held[stage, 0] + z_recv[stage, 0].astype(jnp.float32), y_send, y_recv, 0, 2,
            to_y,
        )

    def deliver(stage):
        column = (col if stage == 0 else 1 - col) * side
        for at, one, two in ((0, y_recv, z_recv), (1, z_recv, y_recv)):
            way = at
            arrived(one.at[stage, 1], link_sems, (way, stage, 1))
            arrived(two.at[stage, 2], link_sems, (1 - way, stage, 2))
            columns = pl.ds(pl.multiple_of(column + at * slim, slim), slim)
            early = first_cols[:, :, columns].reshape(rows_all, slim).astype(jnp.float32)
            whole = kept[stage, :, at * slim : (at + 1) * slim]
            whole = whole + one[stage, 1].astype(jnp.float32) + two[stage, 2].astype(jnp.float32)
            result[:, columns] = (early + 0.5 * whole).astype(jnp.bfloat16)
            written = pltpu.make_async_copy(
                result.at[:, columns], out_ref.at[:, columns], local_sems.at[16 + 2 * stage + at]
            )
            written.start()
            writes.append(written)

    multiply(0)
    forward(0)
    gathered(2)
    gathered(3)
    multiply(1)
    forward(1)
    for slot, owner in ((0, mate), (1, across), (2, corner)):
        arrived(first_cols.at[owner], first_sems, (slot,))
    writes = []
    for lane, count_out in ((0, depth - 1), (3, depth)):
        all_left(lane, gate_w.at[: count_out * high, :])
        all_left(lane + 1, up_w.at[: count_out * high, :])
        all_left(lane + 2, down_w.at[:count_out])
    all_left(6, normed.at[:7])
    all_left(7, part_send)
    for step in range(1, depth):

        @pl.when(row + step < depth)
        def _():
            for copy in plane_copies(step):
                copy.wait_send()

    for copy in sent:
        copy.wait_send()
    deliver(0)
    deliver(1)
    for lane, whole in ((8, to_core), (9, y_send), (10, z_send)):
        all_left(lane, whole)
    for copy in writes:
        copy.wait()


def paired(logs, cell_inputs, rows_inputs, weights):
    ranks, count = lax.axis_size("sp"), lax.axis_size("tp")
    heads = logs[0].shape[0]
    residual, out_gain, in_gain = rows_inputs
    projection, gate_weight, up_weight, down_weight = weights
    rows, width = residual.shape
    inner = projection.shape[0]
    half = gate_weight.shape[1] // 2
    cols = width // count
    block, side, depth = rows // count, cols // 2, ranks // 2
    dma = pltpu.SemaphoreType.DMA

    def low(*shape):
        return pltpu.VMEM(shape, jnp.bfloat16)

    def full(*shape):
        return pltpu.VMEM(shape, jnp.float32)

    like = lambda array: pltpu.VMEM(array.shape, array.dtype)
    members = 2 * count
    operands = (*logs, *cell_inputs, residual, out_gain, in_gain, *weights)
    return pl.pallas_call(
        functools.partial(pair_kernel, ranks, count, heads),
        out_shape=jax.ShapeDtypeStruct((rows, cols), jnp.bfloat16),
        in_specs=[ANY] * len(operands),
        out_specs=ANY,
        scratch_shapes=[
            *(like(array) for array in (*logs, *cell_inputs)),
            low(block, width), full(1, width), full(1, width),
            low(inner, width), low(inner, width),
            low(width, half), low(width, half), low(ranks, half, down_weight.shape[1]),
            full(heads, rows), full(rows, 128),
            full(heads, DQK, DV), low(heads, DQK, DV), full(heads, 8, DQK),
            low(DQK, DV), full(8, DQK),
            full(DQK, DV), full(8, DQK),
            low(DQK, DV), full(8, DQK),
            low(depth - 1, DQK, DV), full(depth - 1, 8, DQK),
            full(DQK, DV), full(8, DQK),
            low(DQK, DV), full(8, DQK),
            low(heads, DQK, DV), full(heads, 8, DQK),
            full(rows, inner), low(rows, inner), low(2, block, inner),
            low(count, block, cols), low(count, block, cols), full(block, width),
            low(block, width), low(count, block, cols),
            low(members, block, width), low(members, block, half),
            low(2, 4, rows, side), low(2, 4, rows, side),
            *(low(2, 3, rows, side // 2) for _ in range(4)),
            full(4, rows, side), full(2, 2, rows, side // 2), full(2, rows, side),
            low(rows, cols),
            dma((20,)), dma((4, 2, depth)), dma((2, 4)), dma((2, 2, depth - 1)), dma((2, 3)),
            dma((count,)), dma((7, 2)), dma((2, 3)), dma((2, 4)), dma((2, 2, 3)), dma((11,)),
        ],
        compiler_params=pltpu.CompilerParams(
            collective_id=0, has_side_effects=True, vmem_limit_bytes=VMEM_BYTES
        ),
        name="layer",
    )(*operands)


def body(
    residual,
    query_matrix,
    key_matrix,
    value_matrix,
    output_gate_logit,
    input_gate_log,
    forget_gate_logit,
    extra_head_decay,
    head_norm_gain,
    projection,
    cell_output_gain,
    mixer_input_gain,
    mixer_gate_weight,
    mixer_up_weight,
    mixer_down_weight,
):
    heads_here = input_gate_log.shape[1]
    if (lax.axis_size("sp"), lax.axis_size("tp"), heads_here) == (8, 4, 2):
        return paired(
            (forget_gate_logit.T, extra_head_decay.T, input_gate_log.T),
            (query_matrix, key_matrix, value_matrix, output_gate_logit, head_norm_gain[None]),
            (residual, cell_output_gain[None], mixer_input_gain[None]),
            (projection, mixer_gate_weight, mixer_up_weight, mixer_down_weight),
        )
    key_low = heads_first(key_matrix, heads_here, DQK)
    value_low = heads_first(value_matrix, heads_here, DV)
    keyed = key_low.astype(jnp.float32)
    valued = value_low.astype(jnp.float32)
    in_logs = input_gate_log.T
    running_log_total = jnp.cumsum(
        (jax.nn.log_sigmoid(forget_gate_logit) + extra_head_decay).T, axis=-1
    )
    zero_memory = jnp.zeros((heads_here, DV, DQK), jnp.float32)
    zero_normalizer = jnp.zeros((heads_here, DQK), jnp.float32)
    lowest = jnp.full((heads_here,), LOWEST_LOG, jnp.float32)
    local_memory, local_normalizer, local_max = fold_state(
        keyed, valued, in_logs, running_log_total, zero_memory, zero_normalizer, lowest
    )
    return layer(
        (running_log_total[:, -1], local_memory, local_normalizer, local_max),
        (running_log_total, in_logs),
        (query_matrix, key_matrix, value_matrix, output_gate_logit, head_norm_gain[None]),
        residual,
        (cell_output_gain[None], mixer_input_gain[None]),
        (projection, mixer_gate_weight, mixer_up_weight, mixer_down_weight),
    )


def solution(mesh):
    return jax.shard_map(
        body,
        mesh=mesh,
        in_specs=(
            P("sp", None),
            P("sp", "tp"),
            P("sp", "tp"),
            P("sp", "tp"),
            P("sp", "tp"),
            P("sp", "tp"),
            P("sp", "tp"),
            P("sp", "tp"),
            P("tp"),
            P("tp", None),
            P(),
            P(),
            P("sp", "tp"),
            P("sp", "tp"),
            P("tp", "sp"),
        ),
        out_specs=P("sp", "tp"),
        check_vma=False,
    )
```
